256 devices in a mesh: sp: 64 (over z, x, core), tp: 4 (over y).
Axes of the slice: x: 4, y: 4, z: 8, core: 2. Of those that a mesh axis runs over, the one named last changes fastest.
Arguments:
- out_cotangent: bfloat16 [16384, 2048], P('sp'), may hold values from -16 to 16
- stream: bfloat16 [16384, 2048], P('sp'), may hold values from -6 to 6
- route_ids: int32 [16384, 2], P('sp'), may hold values from 0 to 63, all different within a row; in each aligned block of 256 rows (0 to 255, 256 to 511, ...) at most 16 rows name the same one
- route_weights: float32 [16384, 2], P('sp'), may hold values from 0.3 to 2
- gate_proj: bfloat16 [64, 2048, 1024], P('sp', None, 'tp'), may hold values from -0.125 to 0.125
- up_proj: bfloat16 [64, 2048, 1024], P('sp', None, 'tp'), may hold values from -0.125 to 0.125
- down_proj: bfloat16 [64, 1024, 2048], P('sp', 'tp'), may hold values from -0.1875 to 0.1875
- outer_gate: bfloat16 [16384, 512], P('sp', 'tp'), may hold values from -6 to 6
- inner_gate: bfloat16 [16384, 512], P('sp', 'tp'), may hold values from -6 to 6
- conv_input: bfloat16 [16384, 512], P('sp', 'tp'), may hold values from -6 to 6
- conv_taps: float32 [3, 512], P(None, 'tp'), may hold values from -4 to 4
- out_proj: bfloat16 [2048, 512], P(None, 'tp'), may hold values from -0.25 to 0.25
Outputs:
- grad_gate_proj: bfloat16 [64, 2048, 1024], P('sp', None, 'tp')
- grad_up_proj: bfloat16 [64, 2048, 1024], P('sp', None, 'tp')
- grad_down_proj: bfloat16 [64, 1024, 2048], P('sp', 'tp')
- grad_out_proj: float32 [2048, 512], P('sp', 'tp')
- grad_outer_gate: float32 [16384, 512], P('sp', 'tp')
- grad_inner_gate: float32 [16384, 512], P('sp', 'tp')
- grad_conv_input: float32 [16384, 512], P('sp', 'tp')
The draws below stay inside these ranges and needn't reach their ends.
Inputs may be any that keep to these rules, and one draw needn't show every extreme that they name: `route_ids`: the 2 experts of a token differ. Among the tokens of one index of sp, no expert is chosen more than 16 times, and in every draw some expert is chosen exactly 16 times by them.
All inputs are finite; a program needn't handle non-finite values.
Results may differ from the reference program's by a relative error of at most 0.018.
Values may be sent and summed in bfloat16 or wider, within the bound.
A program may use at most 64 MiB of HBM per device.

```python
import math
import jax
import jax.numpy as jnp
import numpy as np
from jax import lax

D = 2048
FF = 1024
CONV = 512
TAPS = 3
TOPK = 2
TOK_DEV = 256
EXPERTS = 64
CAP = 16
SLOTS = 1024
TOKENS = 16384
N_TP = 4


def with_spikes(entries, rng, source, target, shards_of, factor):
    owner, partner = [(jnp.arange(entries.shape[dim]) // (entries.shape[dim] // shards_of)).reshape([-1 if axis == dim else 1 for axis in range(entries.ndim)]) for dim in (source, target)]
    chosen = jax.random.permutation(rng, shards_of)[partner]
    strong = (owner == chosen) | (owner == (partner + shards_of // 2) % shards_of)
    return jnp.where(strong, factor * entries, entries)


def block_levels(stream_key, dims, cuts, low, largest):
    def one(dim, parts):
        heights = jax.random.uniform(jax.random.fold_in(jax.random.fold_in(stream_key, 6), dim), (parts,), jnp.float32, low / len(cuts), largest / len(cuts))
        return jnp.repeat(jnp.exp(heights), dims[dim] // parts).reshape((-1,) + (1,) * (len(dims) - dim - 1))

    gain = one(*cuts[0])
    for cut in cuts[1:]:
        gain = gain * one(*cut)
    return gain


def deal_out(own_key, own, number, rows, count, top, reach, lean):
    sequence = jax.random.permutation(own_key, count)
    heavy_load, ordinary = shares(count, rows * top, reach, lean, True), shares(count, rows * top, reach, lean, False)
    places = jnp.arange(count)

    def named(tallies, turn):
        used = int((tallies > 0).sum())
        fixed = max(1, used // 4)
        moved = fixed + (places - fixed + turn * (used - fixed)) % max(1, count - fixed)
        return jnp.zeros((count,), jnp.int32).at[sequence[jnp.where(places < fixed, places, moved)]].set(jnp.asarray(tallies, jnp.int32))

    tallies = jnp.where(number % 4 == 0, named(heavy_load, number // 4), named(ordinary, number - number // 4 - 1))
    mixed = jax.random.permutation(jax.random.fold_in(own, 3), count)
    donor, sink = mixed[0:count // 2 * 2:2], mixed[1:count // 2 * 2:2]
    room = jnp.minimum(tallies[donor] - 1, reach - tallies[sink]) // 2
    room = jnp.where((donor == sequence[0]) | (sink == sequence[0]) | (tallies[sink] == 0), 0, jnp.maximum(room, 0))
    moved = jax.random.randint(jax.random.fold_in(own, 4), (count // 2,), 0, 1 << 20) % (room + 1)
    tallies = tallies.at[donor].add(-moved).at[sink].add(moved)
    labels = jnp.searchsorted(jnp.cumsum(tallies), jnp.arange(rows * top), side="right").astype(jnp.int32)
    table = labels.reshape(top, rows).T
    table = table[jax.random.permutation(jax.random.fold_in(own, 1), rows)]
    turn = jax.random.randint(jax.random.fold_in(own, 2), (rows, 1), 0, top)
    return jnp.take_along_axis(table, (jnp.arange(top)[None, :] + turn) % top, axis=1)


def shares(number_of, total, reach, skew, full):
    portions = [(1 << 20) // math.isqrt(grade ** skew) + 1 for grade in range(1, number_of + 1)]
    largest = reach if full else min(reach, max(-(-total // number_of), total * portions[0] // sum(portions)))
    least = 1 if total - largest >= number_of - 1 else 0
    counts, rest = [largest] + [least] * (number_of - 1), total - largest - least * (number_of - 1)
    while rest > 0:
        movable = [i for i in range(1, number_of) if counts[i] < largest] or [i for i in range(1, number_of) if counts[i] < reach]
        whole, left = sum([portions[i] for i in movable]), rest
        for i in movable:
            more = min(reach - counts[i], max(1, left * portions[i] // whole), rest)
            counts[i] = counts[i] + more
            rest = rest - more
    return np.array(counts)


def bell_draw(own_key, dims, deviation, bound, cuts=(), kind=jnp.bfloat16):
    loudness = block_levels(own_key, dims, cuts, -0.22, 0.18) if cuts else 1.0
    entries = jax.random.normal(own_key, dims, jnp.float32) * deviation * loudness
    return jnp.minimum(jnp.maximum(entries, -bound), bound).astype(kind)


def bell_draw_with(stream_key, extent, width, most, cuts, heavy, kind=jnp.bfloat16):
    values = width * jax.random.normal(stream_key, extent, jnp.float32)
    if cuts:
        values = values * block_levels(stream_key, extent, cuts, -0.22, 0.18)
    return jnp.clip(with_spikes(values, jax.random.fold_in(stream_key, 3), *heavy), -most, most).astype(kind)


def setup_inputs(seed: int = 0) -> dict:
    seeds = jax.random.split(jax.random.key(seed), 13)
    out_cotangent = bell_draw_with(seeds[0], (TOKENS, D), 1.0, 16.0, ((0, 64),), (0, 1, 64, 4.0))
    stream = bell_draw(seeds[1], (TOKENS, D), 1.0, 6.0, ((0, 64),))
    route_ids_keys = jax.random.split(jax.random.fold_in(seeds[2], 1), TOKENS // TOK_DEV)
    route_ids_turns = jax.random.permutation(jax.random.fold_in(seeds[2], 3), TOKENS // TOK_DEV)
    route_ids = jax.vmap(lambda own, number: deal_out(jax.random.fold_in(seeds[2], 2), own, number, TOK_DEV, EXPERTS, TOPK, CAP, 1))(route_ids_keys, route_ids_turns).reshape((TOKENS, TOPK))
    route_weights = jnp.clip(0.3 + 1.7 * jax.random.uniform(seeds[3], (TOKENS, TOPK), jnp.float32) ** block_levels(seeds[3], (TOKENS, TOPK), ((0, 64),), -0.2, 0.2), 0.3, 2.0)
    gate_proj = bell_draw(seeds[4], (EXPERTS, D, FF), D ** -0.5, 0.125, ((0, 64), (2, 4)))
    up_proj = bell_draw(seeds[5], (EXPERTS, D, FF), D ** -0.5, 0.125, ((0, 64), (2, 4)))
    down_proj = bell_draw(seeds[6], (EXPERTS, FF, D), FF ** -0.5, 0.1875, ((0, 64), (1, 4)))
    outer_gate = bell_draw(seeds[7], (TOKENS, CONV), 1.0, 6.0, ((0, 64), (1, 4)))
    inner_gate = bell_draw(seeds[8], (TOKENS, CONV), 1.0, 6.0, ((0, 64), (1, 4)))
    conv_input = bell_draw(seeds[9], (TOKENS, CONV), 1.0, 6.0, ((0, 64), (1, 4)))
    conv_taps = bell_draw(seeds[10], (TAPS, CONV), 0.6, 4.0, ((1, 4),), jnp.float32)
    out_proj = bell_draw(seeds[11], (D, CONV), CONV ** -0.5, 0.25, ((1, 4),))
    return dict(out_cotangent=out_cotangent, stream=stream, route_ids=route_ids, route_weights=route_weights, gate_proj=gate_proj, up_proj=up_proj, down_proj=down_proj, outer_gate=outer_gate, inner_gate=inner_gate, conv_input=conv_input, conv_taps=conv_taps, out_proj=out_proj)


def expert_backward(out_cotangent, stream, route_ids, route_weights, w_gate, w_up, w_down, expert):
    chosen = route_ids == expert
    weight = jnp.sum(jnp.where(chosen, route_weights, 0.0), axis=1)
    hit = jnp.any(chosen, axis=1)
    index = jnp.nonzero(hit, size=SLOTS, fill_value=0)[0].astype(jnp.int32)
    count = jnp.sum(hit.astype(jnp.int32))
    valid = jnp.arange(SLOTS, dtype=jnp.int32) < count
    rows_input = jnp.where(valid[:, None], stream[index], jnp.zeros((), jnp.bfloat16))
    rows_grad = (weight[index][:, None] * out_cotangent[index].astype(jnp.float32))
    rows_grad = jnp.where(valid[:, None], rows_grad, 0.0).astype(jnp.bfloat16)
    gate = jnp.dot(rows_input, w_gate, preferred_element_type=jnp.float32)
    up = jnp.dot(rows_input, w_up, preferred_element_type=jnp.float32)
    sig = jax.nn.sigmoid(gate)
    silu_gate = gate * sig
    hidden = (silu_gate * up).astype(jnp.bfloat16)
    d_hidden = lax.dot_general(rows_grad, w_down, (((1,), (1,)), ((), ())), preferred_element_type=jnp.float32)
    d_gate = (d_hidden * up * sig * (1.0 + gate * (1.0 - sig))).astype(jnp.bfloat16)
    d_up = (d_hidden * silu_gate).astype(jnp.bfloat16)
    over_rows = (((0,), (0,)), ((), ()))
    grad_down = lax.dot_general(hidden, rows_grad, over_rows, preferred_element_type=jnp.float32).astype(jnp.bfloat16)
    grad_gate = lax.dot_general(rows_input, d_gate, over_rows, preferred_element_type=jnp.float32).astype(jnp.bfloat16)
    grad_up = lax.dot_general(rows_input, d_up, over_rows, preferred_element_type=jnp.float32).astype(jnp.bfloat16)
    block = FF // N_TP
    gate_blocks = d_gate.astype(jnp.float32).reshape(SLOTS, N_TP, block)
    up_blocks = d_up.astype(jnp.float32).reshape(SLOTS, N_TP, block)
    wg_blocks = w_gate.astype(jnp.float32).reshape(D, N_TP, block)
    wu_blocks = w_up.astype(jnp.float32).reshape(D, N_TP, block)
    partials = jnp.einsum('snf,dnf->nsd', gate_blocks, wg_blocks) + jnp.einsum('snf,dnf->nsd', up_blocks, wu_blocks)
    partials = partials.astype(jnp.bfloat16).astype(jnp.float32)
    row_grad = jnp.sum(partials, axis=0).astype(jnp.bfloat16)
    row_grad = jnp.where(valid[:, None], row_grad.astype(jnp.float32), 0.0)
    return index, row_grad, grad_gate, grad_up, grad_down


def reference(out_cotangent, stream, route_ids, route_weights, gate_proj, up_proj, down_proj,
              outer_gate, inner_gate, conv_input, conv_taps, out_proj):
    def step(carry, inputs):
        w_gate, w_up, w_down, expert = inputs
        index, row_grad, grad_gate, grad_up, grad_down = expert_backward(
            out_cotangent, stream, route_ids, route_weights, w_gate, w_up, w_down, expert)
        carry = carry.at[index].add(row_grad)
        return carry, (grad_gate, grad_up, grad_down)

    moe_grad, grads = lax.scan(step, jnp.zeros((TOKENS, D), jnp.float32),
                               (gate_proj, up_proj, down_proj, jnp.arange(EXPERTS, dtype=jnp.int32)))
    grad_gate_proj, grad_up_proj, grad_down_proj = grads
    stream_grad = (out_cotangent.astype(jnp.float32) + moe_grad).astype(jnp.bfloat16)
    mixed = inner_gate.astype(jnp.float32) * conv_input.astype(jnp.float32)
    padded = jnp.concatenate([jnp.zeros((2, CONV), jnp.float32), mixed], axis=0)
    conv_out = conv_taps[0] * padded[:TOKENS] + conv_taps[1] * padded[1:TOKENS + 1] + conv_taps[2] * padded[2:]
    mixer_out = (outer_gate.astype(jnp.float32) * conv_out).astype(jnp.bfloat16)
    d_mixer = jnp.dot(stream_grad, out_proj, preferred_element_type=jnp.float32)
    grad_outer_gate = d_mixer * conv_out
    d_conv = d_mixer * outer_gate.astype(jnp.float32)
    trailing = jnp.concatenate([d_conv, jnp.zeros((2, CONV), jnp.float32)], axis=0)
    d_mixed = conv_taps[2] * trailing[:TOKENS] + conv_taps[1] * trailing[1:TOKENS + 1] + conv_taps[0] * trailing[2:]
    grad_inner_gate = d_mixed * conv_input.astype(jnp.float32)
    grad_conv_input = d_mixed * inner_gate.astype(jnp.float32)
    grad_out_proj = lax.dot_general(stream_grad, mixer_out, (((0,), (0,)), ((), ())), preferred_element_type=jnp.float32)
    return (grad_gate_proj, grad_up_proj, grad_down_proj, grad_out_proj,
            grad_outer_gate, grad_inner_gate, grad_conv_input)
```

```python
import functools

import jax
import jax.numpy as jnp
from jax import lax
from jax.experimental import pallas as pl
from jax.experimental.pallas import tpu as pltpu
from jax.sharding import PartitionSpec as P

MESH = pl.DeviceIdType.MESH
F32 = jnp.float32
BF16 = jnp.bfloat16
NY = 4


def plane_size(sp):
    return 8 if sp % 8 == 0 and sp > 8 else 2


def offsets(n):
    out = []
    for d in range(1, n // 2 + 1):
        out.append(d)
        if n - d != d:
            out.append(n - d)
    return out


def remote(src, dst, send, recv, where):
    return pltpu.make_async_remote_copy(
        src_ref=src, dst_ref=dst, send_sem=send, recv_sem=recv, device_id=where, device_id_type=MESH
    )


class Place:
    def __init__(self, sp_size):
        self.plane = plane_size(sp_size)
        self.depth = sp_size // self.plane
        self.sp = lax.axis_index("sp")
        self.y = lax.axis_index("tp")
        self.z = self.sp // self.plane
        self.a = self.sp % self.plane
        self.up = (self.y + 1) % NY
        self.down = (self.y + NY - 1) % NY
        self.across = (self.y + 2) % NY
        self.dz = offsets(self.depth)
        self.da = list(range(1, self.plane))

    def in_z(self, d):
        return (((self.z + d) % self.depth) * self.plane + self.a, self.y)

    def in_plane(self, d):
        return (self.z * self.plane + (self.a + d) % self.plane, self.y)

    def in_y(self, y):
        return (self.sp, y)

    def meet(self, partners):
        barrier = pltpu.get_barrier_semaphore()
        for where in partners:
            pl.semaphore_signal(barrier, inc=1, device_id=where, device_id_type=MESH)
        pl.semaphore_wait(barrier, len(partners))

    def all_partners(self):
        return (
            [self.in_z(d) for d in self.dz]
            + [self.in_plane(d) for d in self.da]
            + [self.in_y(self.up), self.in_y(self.down)]
        )


def dispatch_kernel(sp_size, snd, rows, zbuf, zs, zr, xs, xr, ys, yr):
    me = Place(sp_size)
    plane, depth = me.plane, me.depth
    cap, quarter = snd.shape[3], snd.shape[4]
    chunk = plane * cap
    me.meet(me.all_partners())

    def columns(y):
        return pl.ds(pl.multiple_of(y * quarter, quarter), quarter)

    sent = []
    along_z = []
    for i, d in enumerate(me.dz):
        copy = remote(snd.at[(me.z + d) % depth], zbuf.at[i], zs.at[i], zr.at[i], me.in_z(d))
        copy.start()
        along_z.append(copy)
        sent.append(copy)

    in_plane = {}

    def spread(i):
        if i == 0:
            block = snd.at[me.z]
        else:
            along_z[i - 1].wait_recv()
            block = zbuf.at[i - 1]
        for j, d in enumerate(me.da):
            target = (me.a + d) % plane
            place = pl.ds((i * plane + d) * cap, cap)
            copy = remote(
                block.at[target],
                rows.at[:, place, columns(me.y)],
                xs.at[i, j],
                xr.at[i, j],
                me.in_plane(d),
            )
            copy.start()
            in_plane[i, j] = copy
            sent.append(copy)
        rows[:, pl.ds(i * chunk, cap), columns(me.y)] = block[me.a]

    direct = {}

    def round_y(i):
        for j in range(len(me.da)):
            in_plane[i, j].wait_recv()
        here = rows.at[:, pl.ds(i * chunk, chunk), columns(me.y)]
        for j, y in enumerate((me.up, me.down)):
            copy = remote(here, here, ys.at[i, j], yr.at[i, j], me.in_y(y))
            copy.start()
            direct[i, j] = copy
            sent.append(copy)

    relayed = {}

    def relay(i):
        for j, (origin, target) in enumerate(((me.down, me.up), (me.up, me.down))):
            direct[i, j].wait_recv()
            piece = rows.at[j, pl.ds(i * chunk, chunk), columns(origin)]
            copy = remote(piece, piece, ys.at[i, 2 + j], yr.at[i, 2 + j], me.in_y(target))
            copy.start()
            relayed[i, j] = copy
            sent.append(copy)

    def finish(i):
        for j in range(2):
            relayed[i, j].wait_recv()

    for step in range(depth + 4):
        if step < depth:
            spread(step)
        if 0 <= step - 1 < depth:
            round_y(step - 1)
        if 0 <= step - 3 < depth:
            relay(step - 3)
        if 0 <= step - 4 < depth:
            finish(step - 4)
    for copy in sent:
        copy.wait_send()


def dispatch(snd, sp_size):
    depth, plane, _, cap, quarter = snd.shape
    rows = depth * plane * cap
    dma = pltpu.SemaphoreType.DMA
    return pl.pallas_call(
        functools.partial(dispatch_kernel, sp_size),
        name="dispatch",
        out_shape=jax.ShapeDtypeStruct((2, rows, NY * quarter), BF16),
        in_specs=[pl.BlockSpec(memory_space=pltpu.VMEM)],
        out_specs=pl.BlockSpec(memory_space=pltpu.VMEM),
        scratch_shapes=[
            pltpu.VMEM((depth - 1, plane, 2, cap, quarter), BF16),
            dma((depth - 1,)),
            dma((depth - 1,)),
            dma((depth, plane - 1)),
            dma((depth, plane - 1)),
            dma((depth, 4)),
            dma((depth, 4)),
        ],
        compiler_params=pltpu.CompilerParams(
            collective_id=0, has_side_effects=True, vmem_limit_bytes=48 * 1024 * 1024
        ),
    )(snd)


def combine_kernel(
    sp_size, part, select, own, out,
    gotup, gotdown, relays, sums, share, retz, ret, moe,
    rs, rr, zs, zr, xs, xr, ys, yr,
):
    me = Place(sp_size)
    plane, depth = me.plane, me.depth
    quarter = own.shape[1]
    cap = part.shape[0] // (depth * plane)
    chunk = plane * cap
    half = chunk // 2
    me.meet(me.all_partners())

    def columns(y):
        return pl.ds(pl.multiple_of(y * quarter, quarter), quarter)

    distances = [0] + me.dz
    order = list(range(depth - 1, -1, -1))
    sent = []
    got = {}

    def first(i):
        low, high = pl.ds(i * chunk, half), pl.ds(i * chunk + half, half)
        lo, hi = pl.ds(0, half), pl.ds(half, half)
        jobs = (
            (0, part.at[low, columns(me.across)], relays.at[i, 0], me.down),
            (1, part.at[high, columns(me.across)], relays.at[i, 1], me.up),
            (2, part.at[high, columns(me.down)], gotup.at[i, hi], me.down),
            (3, part.at[low, columns(me.up)], gotdown.at[i, lo], me.up),
        )
        for j, src, dst, y in jobs:
            copy = remote(src, dst, rs.at[i, j], rr.at[i, j], me.in_y(y))
            copy.start()
            got[i, j] = copy
            sent.append(copy)

    def second(i):
        low, high = pl.ds(i * chunk, half), pl.ds(i * chunk + half, half)
        lo, hi = pl.ds(0, half), pl.ds(half, half)
        got[i, 0].wait_recv()
        sums[i, 0] = (
            part[low, columns(me.down)].astype(F32) + relays[i, 0].astype(F32)
        ).astype(BF16)
        copy = remote(sums.at[i, 0], gotup.at[i, lo], rs.at[i, 4], rr.at[i, 4], me.in_y(me.down))
        copy.start()
        got[i, 4] = copy
        sent.append(copy)
        got[i, 1].wait_recv()
        sums[i, 1] = (
            part[high, columns(me.up)].astype(F32) + relays[i, 1].astype(F32)
        ).astype(BF16)
        copy = remote(sums.at[i, 1], gotdown.at[i, hi], rs.at[i, 5], rr.at[i, 5], me.in_y(me.up))
        copy.start()
        got[i, 5] = copy
        sent.append(copy)

    back = {}

    def third(i):
        for j in range(2, 6):
            got[i, j].wait_recv()
        total = (
            part[pl.ds(i * chunk, chunk), columns(me.y)].astype(F32)
            + gotup[i].astype(F32)
            + gotdown[i].astype(F32)
        ).astype(BF16)
        share[i] = total.reshape(plane, cap, quarter)
        if i > 0:
            d = depth - distances[i]
            copy = remote(share.at[i], retz.at[i - 1], zs.at[i - 1], zr.at[i - 1], me.in_z(d))
            copy.start()
            back[i] = copy
            sent.append(copy)

    spreads = {}

    def fourth(i):
        if i > 0:
            back[i].wait_recv()
            block = retz.at[i - 1]
        else:
            block = share.at[0]
        for d in me.da:
            copy = remote(
                block.at[d], ret.at[i, d], xs.at[i, d - 1], xr.at[i, d - 1],
                me.in_plane(plane - d),
            )
            copy.start()
            spreads[i, d] = copy
            sent.append(copy)
        ret[i, 0] = block[0]

    def fifth(i):
        for d in me.da:
            spreads[i, d].wait_recv()
        place = pl.ds(i * chunk, chunk)
        moe[...] += jnp.dot(
            select[:, place],
            ret[i].reshape(chunk, quarter),
            preferred_element_type=F32,
        )

    moe[...] = own[...].astype(F32)
    first(order[0])
    first(order[1])
    for step in range(depth + 6):
        if step + 2 < depth:
            first(order[step + 2])
        if step < depth:
            second(order[step])
        if 0 <= step - 1 < depth:
            third(order[step - 1])
        if 0 <= step - 3 < depth:
            fourth(order[step - 3])
        if 0 <= step - 4 < depth:
            fifth(order[step - 4])

    parts = ys.shape[0]
    tokens = own.shape[0]
    size = tokens // parts
    out[:, columns(me.y)] = moe[...].astype(BF16)
    direct, relayed = {}, {}
    for k in range(parts):
        here = out.at[pl.ds(k * size, size), columns(me.y)]
        for j, y in enumerate((me.up, me.down)):
            copy = remote(here, here, ys.at[k, j], yr.at[k, j], me.in_y(y))
            copy.start()
            direct[k, j] = copy
            sent.append(copy)
    for k in range(parts):
        for j, (origin, target) in enumerate(((me.down, me.up), (me.up, me.down))):
            direct[k, j].wait_recv()
            piece = out.at[pl.ds(k * size + j * (size // 2), size // 2), columns(origin)]
            copy = remote(piece, piece, ys.at[k, 2 + j], yr.at[k, 2 + j], me.in_y(target))
            copy.start()
            relayed[k, j] = copy
            sent.append(copy)
    for k in range(parts):
        for j in range(2):
            relayed[k, j].wait_recv()
    for copy in sent:
        copy.wait_send()


def combine(part, select, own, sp_size):
    plane = plane_size(sp_size)
    depth = sp_size // plane
    tokens, quarter = own.shape
    slots = part.shape[0]
    cap = slots // sp_size
    chunk = plane * cap
    parts = 4
    dma = pltpu.SemaphoreType.DMA
    return pl.pallas_call(
        functools.partial(combine_kernel, sp_size),
        name="combine",
        out_shape=jax.ShapeDtypeStruct((tokens, NY * quarter), BF16),
        in_specs=[pl.BlockSpec(memory_space=pltpu.VMEM)] * 3,
        out_specs=pl.BlockSpec(memory_space=pltpu.VMEM),
        scratch_shapes=[
            pltpu.VMEM((depth, chunk, quarter), BF16),
            pltpu.VMEM((depth, chunk, quarter), BF16),
            pltpu.VMEM((depth, 2, chunk // 2, quarter), BF16),
            pltpu.VMEM((depth, 2, chunk // 2, quarter), BF16),
            pltpu.VMEM((depth, plane, cap, quarter), BF16),
            pltpu.VMEM((depth - 1, plane, cap, quarter), BF16),
            pltpu.VMEM((depth, plane, cap, quarter), BF16),
            pltpu.VMEM((tokens, quarter), F32),
            dma((depth, 6)),
            dma((depth, 6)),
            dma((depth - 1,)),
            dma((depth - 1,)),
            dma((depth, plane - 1)),
            dma((depth, plane - 1)),
            dma((parts, 4)),
            dma((parts, 4)),
        ],
        compiler_params=pltpu.CompilerParams(
            collective_id=1, has_side_effects=True, vmem_limit_bytes=48 * 1024 * 1024
        ),
    )(part, select, own)


def in_blocks(x, dim, devices):
    before, after = (x.shape[:dim], x.shape[dim + 1 :])
    return jnp.moveaxis(x.reshape(*before, devices, -1, *after), dim, 0)


def summed_on_arrival(x, axis, dim):
    pieces = in_blocks(x, dim, lax.axis_size(axis))
    arrived = lax.all_to_all(pieces, axis, split_axis=0, concat_axis=0, tiled=True)
    return arrived.astype(F32).sum(axis=0)


def passed_along(x, axis, by):
    devices = lax.axis_size(axis)
    pairs = [(i, i + by) for i in range(devices) if 0 <= i + by < devices]
    return lax.ppermute(x, axis, pairs)


def shards(
    out_cotangent,
    stream,
    route_ids,
    route_weights,
    gate_proj,
    up_proj,
    down_proj,
    outer_gate,
    inner_gate,
    conv_input,
    conv_taps,
    out_proj,
):
    sp = lax.axis_size("sp")
    plane = plane_size(sp)
    depth = sp // plane
    tokens, width = stream.shape
    cap = 4 * tokens // sp
    slots = sp * cap
    quarter = width // NY

    ids = route_ids.T
    experts = jnp.arange(sp, dtype=jnp.int32)
    chosen = (ids[:, :, None] == experts).astype(BF16)
    either = chosen[0] + chosen[1]
    row = lax.broadcasted_iota(jnp.int32, (tokens, tokens), 0)
    col = lax.broadcasted_iota(jnp.int32, (tokens, tokens), 1)
    earlier = jnp.dot((col < row).astype(BF16), either, preferred_element_type=F32)
    rank = jnp.sum(chosen.astype(F32) * earlier[None], axis=2).astype(jnp.int32)
    place = ids * cap + rank
    slot = jnp.arange(slots, dtype=jnp.int32)
    hit0 = slot[:, None] == place[0][None, :]
    hit1 = slot[:, None] == place[1][None, :]
    weights = route_weights.T
    slot_weight = jnp.sum(
        jnp.where(hit0, weights[0][None, :], 0.0) + jnp.where(hit1, weights[1][None, :], 0.0), axis=1
    )
    pick = (hit0 | hit1).astype(BF16)
    offset = lax.axis_index("tp") * quarter
    own_cotangent = lax.dynamic_slice_in_dim(out_cotangent, offset, quarter, 1)
    own_stream = lax.dynamic_slice_in_dim(stream, offset, quarter, 1)
    sent_input = jnp.dot(pick, own_stream, preferred_element_type=F32).astype(BF16)
    sent_grad = (
        slot_weight[:, None] * jnp.dot(pick, own_cotangent, preferred_element_type=F32)
    ).astype(BF16)
    snd = jnp.stack(
        [
            sent_input.reshape(depth, plane, cap, quarter),
            sent_grad.reshape(depth, plane, cap, quarter),
        ],
        axis=2,
    )
    got = dispatch(snd, sp)
    rows_input, rows_grad = got[0], got[1]

    w_gate = gate_proj[0]
    w_up = up_proj[0]
    w_down = down_proj[0]
    gate = jnp.dot(rows_input, w_gate, preferred_element_type=F32)
    up = jnp.dot(rows_input, w_up, preferred_element_type=F32)
    sig = jax.nn.sigmoid(gate)
    silu_gate = gate * sig
    hidden = (silu_gate * up).astype(BF16)
    across = (((1,), (1,)), ((), ()))
    d_hidden = lax.dot_general(rows_grad, w_down, across, preferred_element_type=F32)
    d_gate = (d_hidden * up * sig * (1.0 + gate * (1.0 - sig))).astype(BF16)
    d_up = (d_hidden * silu_gate).astype(BF16)
    over_rows = (((0,), (0,)), ((), ()))
    grad_down = lax.dot_general(hidden, rows_grad, over_rows, preferred_element_type=F32).astype(BF16)
    grad_gate = lax.dot_general(rows_input, d_gate, over_rows, preferred_element_type=F32).astype(BF16)
    grad_up = lax.dot_general(rows_input, d_up, over_rows, preferred_element_type=F32).astype(BF16)
    partial_input = (
        lax.dot_general(d_gate, w_gate, across, preferred_element_type=F32)
        + lax.dot_general(d_up, w_up, across, preferred_element_type=F32)
    ).astype(BF16)

    dist = jnp.array([0] + offsets(depth), jnp.int32)
    z = lax.axis_index("sp") // plane
    a = lax.axis_index("sp") % plane
    from_z = (z + dist) % depth
    from_a = (a + jnp.arange(plane, dtype=jnp.int32)) % plane
    expert_of = (from_z[:, None] * plane + from_a[None, :]).reshape(-1)
    slot_at = (expert_of[:, None] * cap + jnp.arange(cap, dtype=jnp.int32)).reshape(-1)
    select = (
        (place[0][:, None] == slot_at[None, :]) | (place[1][:, None] == slot_at[None, :])
    ).astype(BF16)
    stream_grad = combine(partial_input, select, own_cotangent, sp)

    mixed = inner_gate.astype(F32) * conv_input.astype(F32)
    previous = passed_along(mixed[tokens - 2 :], "sp", 1)
    extended = jnp.concatenate([previous, mixed], axis=0)
    conv_out = (
        conv_taps[0] * extended[:tokens]
        + conv_taps[1] * extended[1 : tokens + 1]
        + conv_taps[2] * extended[2:]
    )
    mixer_out = (outer_gate.astype(F32) * conv_out).astype(BF16)
    d_mixer = jnp.dot(stream_grad, out_proj, preferred_element_type=F32)
    grad_outer = d_mixer * conv_out
    d_conv = d_mixer * outer_gate.astype(F32)
    following = passed_along(d_conv[:2], "sp", -1)
    trailing = jnp.concatenate([d_conv, following], axis=0)
    d_mixed = (
        conv_taps[2] * trailing[:tokens]
        + conv_taps[1] * trailing[1 : tokens + 1]
        + conv_taps[0] * trailing[2:]
    )
    grad_inner = d_mixed * conv_input.astype(F32)
    grad_input = d_mixed * inner_gate.astype(F32)
    grad_projection = summed_on_arrival(
        lax.dot_general(stream_grad, mixer_out, over_rows, preferred_element_type=F32).astype(BF16),
        "sp",
        0,
    )
    return (
        grad_gate[None],
        grad_up[None],
        grad_down[None],
        grad_projection,
        grad_outer,
        grad_inner,
        grad_input,
    )


def solution(mesh):
    placed = (
        P("sp", None),
        P("sp", None),
        P("sp", None),
        P("sp", None),
        P("sp", None, "tp"),
        P("sp", None, "tp"),
        P("sp", "tp", None),
        P("sp", "tp"),
        P("sp", "tp"),
        P("sp", "tp"),
        P(None, "tp"),
        P(None, "tp"),
    )
    return jax.shard_map(
        shards,
        mesh=mesh,
        in_specs=placed,
        out_specs=(
            P("sp", None, "tp"),
            P("sp", None, "tp"),
            P("sp", "tp", None),
            P("sp", "tp"),
            P("sp", "tp"),
            P("sp", "tp"),
            P("sp", "tp"),
        ),
        check_vma=False,
    )
```

```python
import functools

import jax
import jax.numpy as jnp
from jax import lax
from jax.experimental import pallas as pl
from jax.experimental.pallas import tpu as pltpu
from jax.sharding import PartitionSpec as P

MESH = pl.DeviceIdType.MESH
F32 = jnp.float32
BF16 = jnp.bfloat16
NY = 4


def plane_size(sp):
    return 8 if sp % 8 == 0 and sp > 8 else 2


def offsets(n):
    out = []
    for d in range(1, n // 2 + 1):
        out.append(d)
        if n - d != d:
            out.append(n - d)
    return out


def remote(src, dst, send, recv, where):
    return pltpu.make_async_remote_copy(
        src_ref=src, dst_ref=dst, send_sem=send, recv_sem=recv, device_id=where, device_id_type=MESH
    )


class Place:
    def __init__(self, sp_size):
        self.plane = plane_size(sp_size)
        self.depth = sp_size // self.plane
        self.sp = lax.axis_index("sp")
        self.y = lax.axis_index("tp")
        self.z = self.sp // self.plane
        self.a = self.sp % self.plane
        self.up = (self.y + 1) % NY
        self.down = (self.y + NY - 1) % NY
        self.across = (self.y + 2) % NY
        self.dz = offsets(self.depth)
        self.da = list(range(1, self.plane))

    def in_z(self, d):
        return (((self.z + d) % self.depth) * self.plane + self.a, self.y)

    def in_plane(self, d):
        return (self.z * self.plane + (self.a + d) % self.plane, self.y)

    def in_y(self, y):
        return (self.sp, y)

    def meet(self, partners):
        barrier = pltpu.get_barrier_semaphore()
        for where in partners:
            pl.semaphore_signal(barrier, inc=1, device_id=where, device_id_type=MESH)
        pl.semaphore_wait(barrier, len(partners))

    def all_partners(self):
        return (
            [self.in_z(d) for d in self.dz]
            + [self.in_plane(d) for d in self.da]
            + [self.in_y(self.up), self.in_y(self.down)]
        )


ORDERS = {
    8: "B0 S0 B1 B2 B3 B4 Y0 B5 B6 B7 S1 S2 R0 Y1 Y2 R1 S3 S4 Y3 Y4 R2 F0 F1 D0 S5 S6 R3 Y5 Y6 R4 "
    "F2 F3 D1 S7 Y7 R5 R6 F4 F5 D2 R7 F6 F7 D3",
    2: "B0 S0 B1 Y0 S1 R0 Y1 R1 F0 F1 D0",
}
NT = (((1,), (1,)), ((), ()))
TN = (((0,), (0,)), ((), ()))


def layer_kernel(
    sp_size,
    cap,
    ids, weights, outer, inner, convin, taps,
    cotangent, stream, w_gate, w_up, w_down, w_out,
    g_gate, g_up, g_down, g_out, g_outer, g_inner, g_convin,
    xq, ctq, scaled, wgu, wd, wo,
    snd, zbuf, rows, hid, dgu, part,
    gotup, gotdown, relays, sums, share, retz, ret, moe, out,
    ext, dext, mixer, conv, gp, cbuf, hx, xbuf, hz, zsum,
    local, zs, zr, xs, xr, ys, yr, rs, rr, bs, br, ps, pr, as_, ar, hs, hr, cs, cr, gs, gr, ts, tr,
):
    me = Place(sp_size)
    plane, depth = me.plane, me.depth
    tokens, quarter = xq.shape
    width = quarter * NY
    hidden = wd.shape[0]
    chunk = plane * cap
    half = chunk // 2
    slots = depth * chunk
    distances = [0] + me.dz
    after, before = ((me.sp + 1) % sp_size, me.y), ((me.sp + sp_size - 1) % sp_size, me.y)
    sent = []

    def columns(y):
        return pl.ds(pl.multiple_of(y * quarter, quarter), quarter)

    def send(src, dst, send_sem, recv_sem, where):
        copy = remote(src, dst, send_sem, recv_sem, where)
        copy.start()
        sent.append(copy)
        return copy

    loads = [
        pltpu.make_async_copy(stream.at[:, columns(me.y)], xq, local.at[0]),
        pltpu.make_async_copy(cotangent.at[:, columns(me.y)], ctq, local.at[1]),
        pltpu.make_async_copy(w_gate, wgu.at[:, pl.ds(0, hidden)], local.at[2]),
        pltpu.make_async_copy(w_up, wgu.at[:, pl.ds(hidden, hidden)], local.at[3]),
        pltpu.make_async_copy(w_down, wd, local.at[4]),
        pltpu.make_async_copy(w_out, wo, local.at[5]),
    ]
    for copy in loads:
        copy.start()

    barrier = pltpu.get_barrier_semaphore()
    partners = me.all_partners() + [after, before]
    for where in partners:
        pl.semaphore_signal(barrier, inc=1, device_id=where, device_id_type=MESH)

    def iota(shape, dim):
        return lax.broadcasted_iota(jnp.int32, shape, dim)

    square = (tokens, tokens)
    row, col = iota(square, 0), iota(square, 1)
    ids_col = ids[...]
    ids_row = lax.dot_general(
        ids_col.astype(F32).astype(BF16), (row == col).astype(F32).astype(BF16), TN, preferred_element_type=F32
    ).astype(jnp.int32)
    by_col = [
        (iota((tokens, sp_size), 1) == ids_col[:, k : k + 1]).astype(F32) for k in range(2)
    ]
    by_row = [
        (iota((sp_size, tokens), 0) == ids_row[k : k + 1, :]).astype(F32) for k in range(2)
    ]
    count_col = jnp.dot(
        (col < row).astype(F32).astype(BF16), (by_col[0] + by_col[1]).astype(BF16),
        preferred_element_type=F32,
    )
    count_row = jnp.dot(
        (by_row[0] + by_row[1]).astype(BF16), (row < col).astype(F32).astype(BF16),
        preferred_element_type=F32,
    )
    place_col, place_row = [], []
    for k in range(2):
        rank = jnp.sum(by_col[k] * count_col, axis=1, keepdims=True).astype(jnp.int32)
        place_col.append(ids_col[:, k : k + 1] * cap + rank)
        rank = jnp.sum(by_row[k] * count_row, axis=0, keepdims=True).astype(jnp.int32)
        place_row.append(ids_row[k : k + 1, :] * cap + rank)

    mixed = inner[...].astype(F32) * convin[...].astype(F32)
    ext[pl.ds(8, tokens), :] = mixed

    loads[0].wait()
    loads[1].wait()
    for k in range(2):
        scaled[pl.ds(k * tokens, tokens), :] = (
            weights[:, k : k + 1] * ctq[...].astype(F32)
        ).astype(BF16)

    pl.semaphore_wait(barrier, len(partners))

    def base(i):
        return ((me.z + distances[i]) % depth) * chunk

    along_z = {}

    def build(i):
        slot = base(i) + iota((chunk, tokens), 0)
        hits = [(slot == place_row[k]).astype(F32) for k in range(2)]
        picked = jnp.dot(
            (hits[0] + hits[1]).astype(BF16), xq[...], preferred_element_type=F32
        ).astype(BF16)
        snd[i, :, 0] = picked.reshape(plane, cap, quarter)
        picked = jnp.dot(
            jnp.concatenate(hits, axis=1).astype(BF16), scaled[...], preferred_element_type=F32
        ).astype(BF16)
        snd[i, :, 1] = picked.reshape(plane, cap, quarter)
        if i > 0:
            along_z[i] = send(
                snd.at[i], zbuf.at[i - 1], zs.at[i - 1], zr.at[i - 1], me.in_z(distances[i])
            )

    in_plane = {}

    def spread(i):
        if i == 0:
            block = snd.at[0]
        else:
            along_z[i].wait_recv()
            block = zbuf.at[i - 1]
        for d in me.da:
            in_plane[i, d] = send(
                block.at[(me.a + d) % plane],
                rows.at[:, pl.ds((i * plane + d) * cap, cap), columns(me.y)],
                xs.at[i, d - 1],
                xr.at[i, d - 1],
                me.in_plane(d),
            )
        rows[:, pl.ds(i * chunk, cap), columns(me.y)] = block[me.a]

    direct, relayed = {}, {}

    def round_y(i):
        for d in me.da:
            in_plane[i, d].wait_recv()
        here = rows.at[:, pl.ds(i * chunk, chunk), columns(me.y)]
        for j, y in enumerate((me.up, me.down)):
            direct[i, j] = send(here, here, ys.at[i, j], yr.at[i, j], me.in_y(y))

    def relay(i):
        for j, (origin, target) in enumerate(((me.down, me.up), (me.up, me.down))):
            direct[i, j].wait_recv()
            piece = rows.at[j, pl.ds(i * chunk, chunk), columns(origin)]
            relayed[i, j] = send(piece, piece, ys.at[i, 2 + j], yr.at[i, 2 + j], me.in_y(target))

    def finish(i):
        for j in range(2):
            relayed[i, j].wait_recv()

    def expert(g):
        if g == 0:
            for k in range(2, 5):
                loads[k].wait()
        here = pl.ds(g * 2 * chunk, 2 * chunk)
        both = jnp.dot(rows[0, here, :], wgu[...], preferred_element_type=F32)
        gate, up = both[:, :hidden], both[:, hidden:]
        d_hidden = lax.dot_general(rows[1, here, :], wd[...], NT, preferred_element_type=F32)
        sig = jax.nn.sigmoid(gate)
        silu = gate * sig
        hid[here, :] = (silu * up).astype(BF16)
        dgu[here, pl.ds(0, hidden)] = (d_hidden * up * sig * (1.0 + gate * (1.0 - sig))).astype(BF16)
        dgu[here, pl.ds(hidden, hidden)] = (d_hidden * silu).astype(BF16)
        part[here, :] = lax.dot_general(
            dgu[here, :], wgu[...], NT, preferred_element_type=F32
        ).astype(BF16)

    jobs = {"B": build, "S": spread, "Y": round_y, "R": relay, "F": finish, "D": expert}
    for name in ORDERS[depth].split():
        jobs[name[0]](int(name[1:]))

    got = {}

    def first(i):
        low, high = pl.ds(i * chunk, half), pl.ds(i * chunk + half, half)
        lo, hi = pl.ds(0, half), pl.ds(half, half)
        for j, src, dst, y in (
            (0, part.at[low, columns(me.across)], relays.at[i, 0], me.down),
            (1, part.at[high, columns(me.across)], relays.at[i, 1], me.up),
            (2, part.at[high, columns(me.down)], gotup.at[i, hi], me.down),
            (3, part.at[low, columns(me.up)], gotdown.at[i, lo], me.up),
        ):
            got[i, j] = send(src, dst, rs.at[i, j], rr.at[i, j], me.in_y(y))

    def second(i):
        low, high = pl.ds(i * chunk, half), pl.ds(i * chunk + half, half)
        lo, hi = pl.ds(0, half), pl.ds(half, half)
        for j, mine, y, dst in (
            (0, low, me.down, gotup.at[i, lo]),
            (1, high, me.up, gotdown.at[i, hi]),
        ):
            got[i, j].wait_recv()
            sums[i, j] = (
                part[mine, columns(y)].astype(F32) + relays[i, j].astype(F32)
            ).astype(BF16)
            got[i, 4 + j] = send(sums.at[i, j], dst, rs.at[i, 4 + j], rr.at[i, 4 + j], me.in_y(y))

    back = {}

    def third(i):
        for j in range(2, 6):
            got[i, j].wait_recv()
        total = (
            part[pl.ds(i * chunk, chunk), columns(me.y)].astype(F32)
            + gotup[i].astype(F32)
            + gotdown[i].astype(F32)
        ).astype(BF16)
        share[i] = total.reshape(plane, cap, quarter)
        if i > 0:
            back[i] = send(
                share.at[i], retz.at[i - 1], bs.at[i - 1], br.at[i - 1],
                me.in_z(depth - distances[i]),
            )

    spreads = {}

    def fourth(i):
        if i > 0:
            back[i].wait_recv()
            block = retz.at[i - 1]
        else:
            block = share.at[0]
        for d in me.da:
            spreads[i, d] = send(
                block.at[d], ret.at[i, me.a], ps.at[i, d - 1], pr.at[i, d - 1],
                me.in_plane(plane - d),
            )
        ret[i, me.a] = block[0]

    def fifth(i):
        for d in me.da:
            spreads[i, d].wait_recv()
        slot = base(i) + iota((tokens, chunk), 1)
        hit = ((slot == place_col[0]) | (slot == place_col[1])).astype(F32).astype(BF16)
        moe[...] += jnp.dot(hit, ret[i].reshape(chunk, quarter), preferred_element_type=F32)

    tiles = depth
    wide = width // tiles

    def weight_grads(t):
        cols = pl.ds(t * wide, wide)
        both = lax.dot_general(rows[0, :, cols], dgu[...], TN, preferred_element_type=F32)
        g_gate[cols, :] = both[:, :hidden].astype(BF16)
        g_up[cols, :] = both[:, hidden:].astype(BF16)
        g_down[:, cols] = lax.dot_general(
            hid[...], rows[1, :, cols], TN, preferred_element_type=F32
        ).astype(BF16)

    def convolution():
        halo.wait_recv()
        ext[pl.ds(0, 8), :] = jnp.where(me.sp == 0, 0.0, ext[pl.ds(0, 8), :])
        conv_out = (
            taps[0:1, :] * ext[pl.ds(6, tokens), :]
            + taps[1:2, :] * ext[pl.ds(7, tokens), :]
            + taps[2:3, :] * ext[pl.ds(8, tokens), :]
        )
        conv[...] = conv_out
        mixer[...] = (outer[...].astype(F32) * conv_out).astype(BF16)

    order = list(range(depth - 1, -1, -1))
    moe[...] = ctq[...].astype(F32)
    first(order[0])
    first(order[1])
    halo = send(ext.at[pl.ds(tokens, 8)], ext.at[pl.ds(0, 8)], hs.at[0], hr.at[0], after)
    for step in range(depth + 1):
        if step + 2 < depth:
            first(order[step + 2])
        if step < depth:
            second(order[step])
        if step >= 1:
            third(order[step - 1])
        if step < tiles:
            weight_grads(step)
        if step == 1:
            convolution()
        if step >= 5:
            fourth(order[step - 5])
        if step >= 6:
            fifth(order[step - 6])
    begun = max(depth + 1 - 5, 0)
    ended = max(depth + 1 - 6, 0)
    for k in range(begun, depth):
        fourth(order[k])
    for k in range(ended, depth):
        fifth(order[k])

    parts = as_.shape[0]
    size = tokens // parts
    out[:, columns(me.y)] = moe[...].astype(BF16)
    nearby, passed = {}, {}
    for k in range(parts):
        here = out.at[pl.ds(k * size, size), columns(me.y)]
        for j, y in enumerate((me.up, me.down)):
            nearby[k, j] = send(here, here, as_.at[k, j], ar.at[k, j], me.in_y(y))
    thin = quarter // 2
    for k in range(parts):
        for j, (origin, target) in enumerate(((me.down, me.up), (me.up, me.down))):
            nearby[k, j].wait_recv()
            lanes = pl.ds(pl.multiple_of(origin * quarter + j * thin, thin), thin)
            piece = out.at[pl.ds(k * size, size), lanes]
            passed[k, j] = send(piece, piece, as_.at[k, 2 + j], ar.at[k, 2 + j], me.in_y(target))
    for k in range(parts):
        for j in range(2):
            passed[k, j].wait_recv()

    core = me.a % 2
    across_x = me.a // 2
    chips = plane // 2
    count = sp_size // 2
    block = gp.shape[2]
    gp[...] = (
        lax.dot_general(out[...], mixer[...], TN, preferred_element_type=F32)
        .astype(BF16)
        .reshape(gp.shape)
    )
    between = send(
        gp.at[:, 1 - core], cbuf, cs.at[0], cr.at[0],
        (me.z * plane + across_x * 2 + 1 - core, me.y),
    )
    loads[5].wait()
    d_mixer = jnp.dot(out[...], wo[...], preferred_element_type=F32)
    g_outer[...] = d_mixer * conv[...]
    dext[pl.ds(0, tokens), :] = d_mixer * outer[...].astype(F32)
    trail = send(dext.at[pl.ds(0, 8)], dext.at[pl.ds(tokens, 8)], hs.at[1], hr.at[1], before)

    between.wait_recv()
    summed = gp[:, core].astype(F32) + cbuf[...].astype(F32)
    hx[...] = summed.astype(BF16).reshape(hx.shape)
    over_x = []
    for d in range(1, chips):
        target = (across_x + d) % chips
        over_x.append(
            send(
                hx.at[:, target], xbuf.at[d - 1], gs.at[d - 1], gr.at[d - 1],
                (me.z * plane + target * 2 + core, me.y),
            )
        )

    trail.wait_recv()
    dext[pl.ds(tokens, 8), :] = jnp.where(me.sp == sp_size - 1, 0.0, dext[pl.ds(tokens, 8), :])
    d_mixed = (
        taps[2:3, :] * dext[pl.ds(0, tokens), :]
        + taps[1:2, :] * dext[pl.ds(1, tokens), :]
        + taps[0:1, :] * dext[pl.ds(2, tokens), :]
    )
    g_inner[...] = d_mixed * convin[...].astype(F32)
    g_convin[...] = d_mixed * inner[...].astype(F32)

    summed = hx[:, across_x].astype(F32)
    for d in range(1, chips):
        over_x[d - 1].wait_recv()
        summed += xbuf[d - 1].astype(F32)
    hz[...] = summed
    over_z = []
    for i, d in enumerate(me.dz):
        over_z.append(send(hz.at[(me.z + d) % depth], zsum.at[i], ts.at[i], tr.at[i], me.in_z(d)))
    total = hz[me.z]
    for i, copy in enumerate(over_z):
        copy.wait_recv()
        total += zsum[i]
    g_out[...] = total
    for copy in sent:
        copy.wait_send()


def shards(
    out_cotangent,
    stream,
    route_ids,
    route_weights,
    gate_proj,
    up_proj,
    down_proj,
    outer_gate,
    inner_gate,
    conv_input,
    conv_taps,
    out_proj,
):
    sp = lax.axis_size("sp")
    plane = plane_size(sp)
    depth = sp // plane
    tokens, width = stream.shape
    cap = 4 * tokens // sp
    chunk = plane * cap
    slots = depth * chunk
    quarter = width // NY
    hidden = gate_proj.shape[2]
    channels = outer_gate.shape[1]
    parts = 4
    block = width // sp
    vmem = pl.BlockSpec(memory_space=pltpu.VMEM)
    hbm = pl.BlockSpec(memory_space=pl.ANY)

    def dma(*shape):
        return pltpu.SemaphoreType.DMA(shape)

    def bf16(*shape):
        return pltpu.VMEM(shape, BF16)

    def f32(*shape):
        return pltpu.VMEM(shape, F32)

    def shape(dims, kind):
        return jax.ShapeDtypeStruct(dims, kind)

    grads = pl.pallas_call(
        functools.partial(layer_kernel, sp, cap),
        name="layer",
        out_shape=(
            shape((width, hidden), BF16),
            shape((width, hidden), BF16),
            shape((hidden, width), BF16),
            shape((block, channels), F32),
            shape((tokens, channels), F32),
            shape((tokens, channels), F32),
            shape((tokens, channels), F32),
        ),
        in_specs=[vmem] * 6 + [hbm] * 6,
        out_specs=(vmem,) * 7,
        scratch_shapes=[
            bf16(tokens, quarter),
            bf16(tokens, quarter),
            bf16(2 * tokens, quarter),
            bf16(width, 2 * hidden),
            bf16(hidden, width),
            bf16(width, channels),
            bf16(depth, plane, 2, cap, quarter),
            bf16(depth - 1, plane, 2, cap, quarter),
            bf16(2, slots, width),
            bf16(slots, hidden),
            bf16(slots, 2 * hidden),
            bf16(slots, width),
            bf16(depth, chunk, quarter),
            bf16(depth, chunk, quarter),
            bf16(depth, 2, chunk // 2, quarter),
            bf16(depth, 2, chunk // 2, quarter),
            bf16(depth, plane, cap, quarter),
            bf16(depth - 1, plane, cap, quarter),
            bf16(depth, plane, cap, quarter),
            f32(tokens, quarter),
            bf16(tokens, width),
            f32(tokens + 8, channels),
            f32(tokens + 8, channels),
            bf16(tokens, channels),
            f32(tokens, channels),
            bf16(sp // 2, 2, block, channels),
            bf16(sp // 2, block, channels),
            bf16(depth, plane // 2, block, channels),
            bf16(max(plane // 2 - 1, 1), depth, block, channels),
            f32(depth, block, channels),
            f32(depth - 1, block, channels),
            dma(6),
            dma(depth - 1),
            dma(depth - 1),
            dma(depth, plane - 1),
            dma(depth, plane - 1),
            dma(depth, 4),
            dma(depth, 4),
            dma(depth, 6),
            dma(depth, 6),
            dma(depth - 1),
            dma(depth - 1),
            dma(depth, plane - 1),
            dma(depth, plane - 1),
            dma(parts, 4),
            dma(parts, 4),
            dma(2),
            dma(2),
            dma(1),
            dma(1),
            dma(max(plane // 2 - 1, 1)),
            dma(max(plane // 2 - 1, 1)),
            dma(depth - 1),
            dma(depth - 1),
        ],
        compiler_params=pltpu.CompilerParams(
            collective_id=0, has_side_effects=True, vmem_limit_bytes=60 * 1024 * 1024
        ),
    )(
        route_ids, route_weights, outer_gate, inner_gate, conv_input, conv_taps,
        out_cotangent, stream, gate_proj[0], up_proj[0], down_proj[0], out_proj,
    )
    return (grads[0][None], grads[1][None], grads[2][None], *grads[3:])


def solution(mesh):
    placed = (
        P("sp", None),
        P("sp", None),
        P("sp", None),
        P("sp", None),
        P("sp", None, "tp"),
        P("sp", None, "tp"),
        P("sp", "tp", None),
        P("sp", "tp"),
        P("sp", "tp"),
        P("sp", "tp"),
        P(None, "tp"),
        P(None, "tp"),
    )
    return jax.shard_map(
        shards,
        mesh=mesh,
        in_specs=placed,
        out_specs=(
            P("sp", None, "tp"),
            P("sp", None, "tp"),
            P("sp", "tp", None),
            P("sp", "tp"),
            P("sp", "tp"),
            P("sp", "tp"),
            P("sp", "tp"),
        ),
        check_vma=False,
    )
```

```python
import functools

import jax
import jax.numpy as jnp
from jax import lax
from jax.experimental import pallas as pl
from jax.experimental.pallas import tpu as pltpu
from jax.sharding import PartitionSpec as P

MESH = pl.DeviceIdType.MESH
F32 = jnp.float32
BF16 = jnp.bfloat16
NY = 4


def plane_size(sp):
    return 8 if sp % 8 == 0 and sp > 8 else 2


def offsets(n):
    out = []
    for d in range(1, n // 2 + 1):
        out.append(d)
        if n - d != d:
            out.append(n - d)
    return out


def remote(src, dst, send, recv, where):
    return pltpu.make_async_remote_copy(
        src_ref=src, dst_ref=dst, send_sem=send, recv_sem=recv, device_id=where, device_id_type=MESH
    )


class Place:
    def __init__(self, sp_size):
        self.plane = plane_size(sp_size)
        self.depth = sp_size // self.plane
        self.sp = lax.axis_index("sp")
        self.y = lax.axis_index("tp")
        self.z = self.sp // self.plane
        self.a = self.sp % self.plane
        self.up = (self.y + 1) % NY
        self.down = (self.y + NY - 1) % NY
        self.across = (self.y + 2) % NY
        self.dz = offsets(self.depth)
        self.da = list(range(1, self.plane))

    def at(self, d, k):
        plane = self.plane
        return (((self.z + d) % self.depth) * plane + (self.a + k) % plane, self.y)

    def in_y(self, y):
        return (self.sp, y)


ORDERS = {
    8: "S0 S1 S2 Y0 S3 S4 Y1 Y2 R0 R1 S5 S6 R2 Y3 Y4 R3 S7 R4 Y5 Y6 R5 X1 X2 X0 Y7 R6 R7 F4 F5 D2 P5 P4 "
    "F2 F3 D1 F6 F7 D3 P7 P6 F0 F1 D0",
    2: "S0 S1 Y0 Y1 R0 X0 R1 F0 F1 D0 P1 P0",
}
NEAR = {8: 3, 2: 1}
RETURNS = {8: (5, 4, 7, 6, 3, 2, 1, 0), 2: (1, 0)}
NT = (((1,), (1,)), ((), ()))
TN = (((0,), (0,)), ((), ()))


def layer_kernel(
    sp_size,
    cap,
    ids, weights, outer, inner, convin, taps,
    cotangent, stream, w_gate, w_up, w_down, w_out,
    g_gate, g_up, g_down, g_out, g_outer, g_inner, g_convin,
    xall, ctq, scaled, wgu, wd, wo,
    snd, wide_snd, rows, hid, dgu, part,
    gotup, gotdown, relays, sums, share, ret, moe, out,
    ext, dext, mixer, conv, gp, cbuf, hx, xbuf, hz, zsum,
    local, xs, xr, ws, wr, ys, yr, rs, rr, ps, pr, as_, ar, hs, hr, cs, cr, gs, gr, ts, tr,
):
    me = Place(sp_size)
    plane, depth = me.plane, me.depth
    tokens, quarter = ctq.shape
    width = quarter * NY
    hidden = wd.shape[0]
    chunk = plane * cap
    half = chunk // 2
    slots = depth * chunk
    distances = [0] + me.dz
    after, before = ((me.sp + 1) % sp_size, me.y), ((me.sp + sp_size - 1) % sp_size, me.y)
    others = [(i, k) for i in range(depth) for k in range(plane) if i + k > 0]
    near = NEAR[depth]
    sent = []
    groups = []

    def columns(y):
        return pl.ds(pl.multiple_of(y * quarter, quarter), quarter)

    def send(src, dst, send_sem, recv_sem, where):
        copy = remote(src, dst, send_sem, recv_sem, where)
        copy.start()
        sent.append(copy)
        return copy

    loads = [
        pltpu.make_async_copy(stream, xall, local.at[0]),
        pltpu.make_async_copy(cotangent.at[:, columns(me.y)], ctq, local.at[1]),
        pltpu.make_async_copy(w_gate, wgu.at[:, pl.ds(0, hidden)], local.at[2]),
        pltpu.make_async_copy(w_up, wgu.at[:, pl.ds(hidden, hidden)], local.at[3]),
        pltpu.make_async_copy(w_down, wd, local.at[4]),
        pltpu.make_async_copy(w_out, wo, local.at[5]),
    ]
    for copy in loads:
        copy.start()

    barrier = pltpu.get_barrier_semaphore()
    partners = [me.at(distances[i], k) for i, k in others] + [me.in_y(me.up), me.in_y(me.down)]
    for where in partners:
        pl.semaphore_signal(barrier, inc=1, device_id=where, device_id_type=MESH)

    def iota(shape, dim):
        return lax.broadcasted_iota(jnp.int32, shape, dim)

    square = (tokens, tokens)
    row, col = iota(square, 0), iota(square, 1)
    ids_row = ids[...]
    upright = [
        jnp.broadcast_to(a[k : k + 1, :], (128, tokens)).T
        for a in (ids_row.astype(F32), weights[...])
        for k in range(2)
    ]
    ids_col = [a[:, :1].astype(jnp.int32) for a in upright[:2]]
    weight_col = [a[:, :1] for a in upright[2:]]
    by_col = [
        (iota((tokens, sp_size), 1) == ids_col[k]).astype(F32) for k in range(2)
    ]
    by_row = [
        (iota((sp_size, tokens), 0) == ids_row[k : k + 1, :]).astype(F32) for k in range(2)
    ]
    count_col = jnp.dot(
        (col < row).astype(F32).astype(BF16), (by_col[0] + by_col[1]).astype(BF16),
        preferred_element_type=F32,
    )
    count_row = jnp.dot(
        (by_row[0] + by_row[1]).astype(BF16), (row < col).astype(F32).astype(BF16),
        preferred_element_type=F32,
    )
    place_col, place_row = [], []
    for k in range(2):
        rank = jnp.sum(by_col[k] * count_col, axis=1, keepdims=True).astype(jnp.int32)
        place_col.append(ids_col[k] * cap + rank)
        rank = jnp.sum(by_row[k] * count_row, axis=0, keepdims=True).astype(jnp.int32)
        place_row.append(ids_row[k : k + 1, :] * cap + rank)

    mixed = inner[...].astype(F32) * convin[...].astype(F32)
    ext[pl.ds(8, tokens), :] = mixed

    loads[0].wait()
    loads[1].wait()
    for k in range(2):
        scaled[pl.ds(k * tokens, tokens), :] = (
            weight_col[k] * ctq[...].astype(F32)
        ).astype(BF16)

    def base(i):
        return ((me.z + distances[i]) % depth) * chunk

    def build(i):
        slot = base(i) + iota((chunk, tokens), 0)
        hits = [(slot == place_row[k]).astype(F32) for k in range(2)]
        both = (hits[0] + hits[1]).astype(BF16)
        if i < near:
            picked = jnp.dot(both, xall[...], preferred_element_type=F32).astype(BF16)
            wide_snd[i] = picked.reshape(plane, cap, width)
        else:
            picked = jnp.dot(both, xall[:, columns(me.y)], preferred_element_type=F32).astype(BF16)
            snd[i, :, 0] = picked.reshape(plane, cap, quarter)
        picked = jnp.dot(
            jnp.concatenate(hits, axis=1).astype(BF16), scaled[...], preferred_element_type=F32
        ).astype(BF16)
        snd[i, :, 1] = picked.reshape(plane, cap, quarter)

    def group(i, sends, out_of, send_sem, recv_sem):
        for k in range(plane):
            if i + k > 0:
                src, dst = sends(k)
                remote(src, dst, send_sem, recv_sem, me.at(*out_of(k))).start()

    def whole(ref, send_sem, recv_sem):
        return remote(ref, ref, send_sem, recv_sem, me.in_y(me.up))

    def block(i, k):
        return pl.ds((i * plane + k) * cap, cap)

    def blocks(i):
        return pl.ds(cap, chunk - cap) if i == 0 else pl.ds(i * chunk, chunk)

    def those(ref, i):
        return ref.at[0, pl.ds(0, plane - 1)] if i == 0 else ref.at[i]

    def outward(i):
        return lambda k: (distances[i], k)

    def ship(i):
        if i < near:
            def sends(k):
                target = (me.a + k) % plane
                return snd.at[i, target, 1], rows.at[1, block(i, k), columns(me.y)]
        else:
            def sends(k):
                target = (me.a + k) % plane
                return snd.at[i, target], rows.at[:, block(i, k), columns(me.y)]
        group(i, sends, outward(i), xs.at[i], xr.at[i])
        ref = snd.at[:, :, 1] if i < near else snd
        groups.append(whole(those(ref, i), xs.at[i], xr.at[i]))
        if i == 0:
            rows[1, pl.ds(0, cap), columns(me.y)] = snd[0, me.a, 1]
            rows[0, pl.ds(0, cap), :] = wide_snd[0, me.a]

    def ship_wide(i):
        def sends(k):
            return wide_snd.at[i, (me.a + k) % plane], rows.at[0, block(i, k), :]

        group(i, sends, outward(i), ws.at[i], wr.at[i])
        groups.append(whole(those(wide_snd, i), ws.at[i], wr.at[i]))

    for i in range(depth):
        build(i)
    pl.semaphore_wait(barrier, len(partners))

    direct, relayed = {}, {}

    def round_y(i):
        arrays = 1 if i < near else slice(None)
        whole(rows.at[arrays, blocks(i), columns(me.y)], xs.at[i], xr.at[i]).wait_recv()
        here = rows.at[arrays, pl.ds(i * chunk, chunk), columns(me.y)]
        for j, y in enumerate((me.up, me.down)):
            direct[i, j] = send(here, here, ys.at[i, j], yr.at[i, j], me.in_y(y))

    def relay(i):
        for j, (origin, target) in enumerate(((me.down, me.up), (me.up, me.down))):
            direct[i, j].wait_recv()
            if i < near:
                piece = rows.at[1, pl.ds(i * chunk + j * half, half), columns(origin)]
            else:
                piece = rows.at[j, pl.ds(i * chunk, chunk), columns(origin)]
            relayed[i, j] = send(piece, piece, ys.at[i, 2 + j], yr.at[i, 2 + j], me.in_y(target))

    def finish(i):
        for j in range(2):
            relayed[i, j].wait_recv()
        if i < near:
            whole(rows.at[0, blocks(i), :], ws.at[i], wr.at[i]).wait_recv()

    ready = []

    def expert(g):
        if not ready:
            ready.append(True)
            for k in range(2, 5):
                loads[k].wait()
        here = pl.ds(g * 2 * chunk, 2 * chunk)
        both = jnp.dot(rows[0, here, :], wgu[...], preferred_element_type=F32)
        gate, up = both[:, :hidden], both[:, hidden:]
        d_hidden = lax.dot_general(rows[1, here, :], wd[...], NT, preferred_element_type=F32)
        sig = jax.nn.sigmoid(gate)
        silu = gate * sig
        hid[here, :] = (silu * up).astype(BF16)
        dgu[here, pl.ds(0, hidden)] = (d_hidden * up * sig * (1.0 + gate * (1.0 - sig))).astype(BF16)
        dgu[here, pl.ds(hidden, hidden)] = (d_hidden * silu).astype(BF16)
        part[here, :] = lax.dot_general(
            dgu[here, :], wgu[...], NT, preferred_element_type=F32
        ).astype(BF16)

    got = {}

    def first(i):
        low, high = pl.ds(i * chunk, half), pl.ds(i * chunk + half, half)
        lo, hi = pl.ds(0, half), pl.ds(half, half)
        for j, src, dst, y in (
            (0, part.at[low, columns(me.across)], relays.at[i, 0], me.down),
            (1, part.at[high, columns(me.across)], relays.at[i, 1], me.up),
            (2, part.at[high, columns(me.down)], gotup.at[i, hi], me.down),
            (3, part.at[low, columns(me.up)], gotdown.at[i, lo], me.up),
        ):
            got[i, j] = send(src, dst, rs.at[i, j], rr.at[i, j], me.in_y(y))

    jobs = {
        "S": ship, "X": ship_wide, "Y": round_y, "R": relay, "F": finish, "D": expert, "P": first,
    }
    for name in ORDERS[depth].split():
        jobs[name[0]](int(name[1:]))

    def second(i):
        low, high = pl.ds(i * chunk, half), pl.ds(i * chunk + half, half)
        lo, hi = pl.ds(0, half), pl.ds(half, half)
        for j, mine, y, dst in (
            (0, low, me.down, gotup.at[i, lo]),
            (1, high, me.up, gotdown.at[i, hi]),
        ):
            got[i, j].wait_recv()
            sums[i, j] = (
                part[mine, columns(y)].astype(F32) + relays[i, j].astype(F32)
            ).astype(BF16)
            got[i, 4 + j] = send(sums.at[i, j], dst, rs.at[i, 4 + j], rr.at[i, 4 + j], me.in_y(y))

    def third(i):
        for j in range(2, 6):
            got[i, j].wait_recv()
        total = (
            part[pl.ds(i * chunk, chunk), columns(me.y)].astype(F32)
            + gotup[i].astype(F32)
            + gotdown[i].astype(F32)
        ).astype(BF16)
        share[i] = total.reshape(plane, cap, quarter)
        if i == 0:
            ret[0, me.a] = share[0, 0]

        def sends(k):
            return share.at[i, k], ret.at[i, me.a]

        group(i, sends, lambda k: (depth - distances[i], plane - k), ps.at[i], pr.at[i])
        groups.append(whole(those(share, i), ps.at[i], pr.at[i]))

    def fourth(i):
        whole(those(ret, i), ps.at[i], pr.at[i]).wait_recv()
        slot = base(i) + iota((tokens, chunk), 1)
        hit = ((slot == place_col[0]) | (slot == place_col[1])).astype(F32).astype(BF16)
        moe[...] += jnp.dot(hit, ret[i].reshape(chunk, quarter), preferred_element_type=F32)

    tiles = depth
    wide = width // tiles

    def weight_grads(t):
        cols = pl.ds(t * wide, wide)
        both = lax.dot_general(rows[0, :, cols], dgu[...], TN, preferred_element_type=F32)
        g_gate[0, cols, :] = both[:, :hidden].astype(BF16)
        g_up[0, cols, :] = both[:, hidden:].astype(BF16)
        g_down[0, :, cols] = lax.dot_general(
            hid[...], rows[1, :, cols], TN, preferred_element_type=F32
        ).astype(BF16)

    def convolution():
        halo.wait_recv()
        ext[pl.ds(0, 8), :] = jnp.where(me.sp == 0, 0.0, ext[pl.ds(0, 8), :])
        conv_out = (
            taps[0:1, :] * ext[pl.ds(6, tokens), :]
            + taps[1:2, :] * ext[pl.ds(7, tokens), :]
            + taps[2:3, :] * ext[pl.ds(8, tokens), :]
        )
        conv[...] = conv_out
        mixer[...] = (outer[...].astype(F32) * conv_out).astype(BF16)

    order = RETURNS[depth]
    moe[...] = ctq[...].astype(F32)
    halo = send(ext.at[pl.ds(tokens, 8)], ext.at[pl.ds(0, 8)], hs.at[0], hr.at[0], after)
    lag = 5
    early = min(4, depth)
    for step in range(depth + 1):
        if step + 2 < depth and step + 2 >= early:
            first(order[step + 2])
        if step < depth:
            second(order[step])
        if step >= 1:
            third(order[step - 1])
        if step < tiles:
            weight_grads(step)
        if step == 1:
            convolution()
        if step >= lag:
            fourth(order[step - lag])
    for k in range(max(depth + 1 - lag, 0), depth):
        fourth(order[k])

    parts = as_.shape[0]
    size = tokens // parts
    out[:, columns(me.y)] = moe[...].astype(BF16)
    nearby, passed = {}, {}
    for k in range(parts):
        here = out.at[pl.ds(k * size, size), columns(me.y)]
        for j, y in enumerate((me.up, me.down)):
            nearby[k, j] = send(here, here, as_.at[k, j], ar.at[k, j], me.in_y(y))
    thin = quarter // 2
    for k in range(parts):
        for j, (origin, target) in enumerate(((me.down, me.up), (me.up, me.down))):
            nearby[k, j].wait_recv()
            lanes = pl.ds(pl.multiple_of(origin * quarter + j * thin, thin), thin)
            piece = out.at[pl.ds(k * size, size), lanes]
            passed[k, j] = send(piece, piece, as_.at[k, 2 + j], ar.at[k, 2 + j], me.in_y(target))
    for k in range(parts):
        for j in range(2):
            passed[k, j].wait_recv()

    core = me.a % 2
    across_x = me.a // 2
    chips = plane // 2
    count = sp_size // 2
    block = gp.shape[2]
    gp[...] = (
        lax.dot_general(out[...], mixer[...], TN, preferred_element_type=F32)
        .astype(BF16)
        .reshape(gp.shape)
    )
    between = send(
        gp.at[:, 1 - core], cbuf, cs.at[0], cr.at[0],
        (me.z * plane + across_x * 2 + 1 - core, me.y),
    )
    loads[5].wait()
    d_mixer = jnp.dot(out[...], wo[...], preferred_element_type=F32)
    g_outer[...] = d_mixer * conv[...]
    dext[pl.ds(0, tokens), :] = d_mixer * outer[...].astype(F32)
    trail = send(dext.at[pl.ds(0, 8)], dext.at[pl.ds(tokens, 8)], hs.at[1], hr.at[1], before)

    between.wait_recv()
    summed = gp[:, core].astype(F32) + cbuf[...].astype(F32)
    hx[...] = summed.astype(BF16).reshape(hx.shape)
    over_x = []
    for d in range(1, chips):
        target = (across_x + d) % chips
        over_x.append(
            send(
                hx.at[:, target], xbuf.at[d - 1], gs.at[d - 1], gr.at[d - 1],
                (me.z * plane + target * 2 + core, me.y),
            )
        )

    trail.wait_recv()
    dext[pl.ds(tokens, 8), :] = jnp.where(me.sp == sp_size - 1, 0.0, dext[pl.ds(tokens, 8), :])
    d_mixed = (
        taps[2:3, :] * dext[pl.ds(0, tokens), :]
        + taps[1:2, :] * dext[pl.ds(1, tokens), :]
        + taps[0:1, :] * dext[pl.ds(2, tokens), :]
    )
    g_inner[...] = d_mixed * convin[...].astype(F32)
    g_convin[...] = d_mixed * inner[...].astype(F32)

    summed = hx[:, across_x].astype(F32)
    for d in range(1, chips):
        over_x[d - 1].wait_recv()
        summed += xbuf[d - 1].astype(F32)
    hz[...] = summed
    over_z = []
    for i, d in enumerate(me.dz):
        over_z.append(send(hz.at[(me.z + d) % depth], zsum.at[i], ts.at[i], tr.at[i], me.at(d, 0)))
    total = hz[me.z]
    for i, copy in enumerate(over_z):
        copy.wait_recv()
        total += zsum[i]
    g_out[...] = total
    for copy in sent + groups:
        copy.wait_send()


def shards(
    out_cotangent,
    stream,
    route_ids,
    route_weights,
    gate_proj,
    up_proj,
    down_proj,
    outer_gate,
    inner_gate,
    conv_input,
    conv_taps,
    out_proj,
):
    sp = lax.axis_size("sp")
    plane = plane_size(sp)
    depth = sp // plane
    tokens, width = stream.shape
    cap = 4 * tokens // sp
    chunk = plane * cap
    slots = depth * chunk
    quarter = width // NY
    hidden = gate_proj.shape[2]
    channels = outer_gate.shape[1]
    parts = 4
    near = NEAR[depth]
    block = width // sp
    vmem = pl.BlockSpec(memory_space=pltpu.VMEM)
    hbm = pl.BlockSpec(memory_space=pl.ANY)

    def dma(*shape):
        return pltpu.SemaphoreType.DMA(shape)

    def bf16(*shape):
        return pltpu.VMEM(shape, BF16)

    def f32(*shape):
        return pltpu.VMEM(shape, F32)

    shapes = (
        ((1, width, hidden), BF16),
        ((1, width, hidden), BF16),
        ((1, hidden, width), BF16),
        ((block, channels), F32),
        ((tokens, channels), F32),
        ((tokens, channels), F32),
        ((tokens, channels), F32),
    )
    return pl.pallas_call(
        functools.partial(layer_kernel, sp, cap),
        name="layer",
        out_shape=tuple(pltpu.VMEM(*s) for s in shapes),
        in_specs=[vmem] * 6 + [hbm] * 6,
        out_specs=(vmem,) * 7,
        scratch_shapes=[
            bf16(tokens, width),
            bf16(tokens, quarter),
            bf16(2 * tokens, quarter),
            bf16(width, 2 * hidden),
            bf16(hidden, width),
            bf16(width, channels),
            bf16(depth, plane, 2, cap, quarter),
            bf16(near, plane, cap, width),
            bf16(2, slots, width),
            bf16(slots, hidden),
            bf16(slots, 2 * hidden),
            bf16(slots, width),
            bf16(depth, chunk, quarter),
            bf16(depth, chunk, quarter),
            bf16(depth, 2, chunk // 2, quarter),
            bf16(depth, 2, chunk // 2, quarter),
            bf16(depth, plane, cap, quarter),
            bf16(depth, plane, cap, quarter),
            f32(tokens, quarter),
            bf16(tokens, width),
            f32(tokens + 8, channels),
            f32(tokens + 8, channels),
            bf16(tokens, channels),
            f32(tokens, channels),
            bf16(sp // 2, 2, block, channels),
            bf16(sp // 2, block, channels),
            bf16(depth, plane // 2, block, channels),
            bf16(max(plane // 2 - 1, 1), depth, block, channels),
            f32(depth, block, channels),
            f32(depth - 1, block, channels),
            dma(6),
            dma(depth),
            dma(depth),
            dma(near),
            dma(near),
            dma(depth, 4),
            dma(depth, 4),
            dma(depth, 6),
            dma(depth, 6),
            dma(depth),
            dma(depth),
            dma(parts, 4),
            dma(parts, 4),
            dma(2),
            dma(2),
            dma(1),
            dma(1),
            dma(max(plane // 2 - 1, 1)),
            dma(max(plane // 2 - 1, 1)),
            dma(depth - 1),
            dma(depth - 1),
        ],
        compiler_params=pltpu.CompilerParams(
            collective_id=0, has_side_effects=True, vmem_limit_bytes=60 * 1024 * 1024
        ),
    )(
        route_ids.T, route_weights.T, outer_gate, inner_gate, conv_input, conv_taps,
        out_cotangent, stream, gate_proj[0], up_proj[0], down_proj[0], out_proj,
    )


def solution(mesh):
    placed = (
        P("sp", None),
        P("sp", None),
        P("sp", None),
        P("sp", None),
        P("sp", None, "tp"),
        P("sp", None, "tp"),
        P("sp", "tp", None),
        P("sp", "tp"),
        P("sp", "tp"),
        P("sp", "tp"),
        P(None, "tp"),
        P(None, "tp"),
    )
    return jax.shard_map(
        shards,
        mesh=mesh,
        in_specs=placed,
        out_specs=(
            P("sp", None, "tp"),
            P("sp", None, "tp"),
            P("sp", "tp", None),
            P("sp", "tp"),
            P("sp", "tp"),
            P("sp", "tp"),
            P("sp", "tp"),
        ),
        check_vma=False,
    )
```

```python
import functools

import jax
import jax.numpy as jnp
from jax import lax
from jax.experimental import pallas as pl
from jax.experimental.pallas import tpu as pltpu
from jax.sharding import PartitionSpec as P

MESH = pl.DeviceIdType.MESH
F32 = jnp.float32
BF16 = jnp.bfloat16
NY = 4


def plane_size(sp):
    return sp // 8


def offsets(n):
    out = []
    for d in range(1, n // 2 + 1):
        out.append(d)
        if n - d != d:
            out.append(n - d)
    return out


def remote(src, dst, send, recv, where):
    return pltpu.make_async_remote_copy(
        src_ref=src, dst_ref=dst, send_sem=send, recv_sem=recv, device_id=where, device_id_type=MESH
    )


class Place:
    def __init__(self, sp_size):
        self.plane = plane_size(sp_size)
        self.depth = sp_size // self.plane
        self.sp = lax.axis_index("sp")
        self.y = lax.axis_index("tp")
        self.z = self.sp // self.plane
        self.a = self.sp % self.plane
        self.up = (self.y + 1) % NY
        self.down = (self.y + NY - 1) % NY
        self.across = (self.y + 2) % NY
        self.dz = offsets(self.depth)
        self.da = list(range(1, self.plane))

    def at(self, d, k):
        plane = self.plane
        return (((self.z + d) % self.depth) * plane + (self.a + k) % plane, self.y)

    def in_y(self, y):
        return (self.sp, y)


ORDERS = {
    8: "S0 S1 S2 W0 Y0 S3 S4 S5 S6 Y1 Y2 R0 C0 R1 S7 X0 R2 Y3 Y4 R3 R4 Y5 Y6 R5 Y7 R6 R7 F4 F5 D2 P5 P4 "
    "F2 F3 D1 F6 F7 D3 F0 F1 D0",
}
NEAR = {8: 1}
RETURNS = {8: (5, 4, 7, 6, 3, 2, 1, 0)}
NT = (((1,), (1,)), ((), ()))
TN = (((0,), (0,)), ((), ()))


def layer_kernel(
    sp_size,
    cap,
    ids, weights, outer, inner, convin, taps,
    cotangent, stream, w_gate, w_up, w_down, w_out,
    g_gate, g_up, g_down, g_out, g_outer, g_inner, g_convin,
    xall, ctq, scaled, wgu, wd, wo,
    snd, wide_snd, rows, hid, dgu, part,
    gotup, gotdown, relays, sums, share, ret, moe, wall, mall, dsend, dgot,
    ext, dext, mixer, conv, gp, cbuf, hx, xbuf, hz, zsum,
    local, xs, xr, ws, wr, ys, yr, rs, rr, ps, pr, as_, ar, hs, hr, cs, cr, gs, gr, ts, tr,
):
    me = Place(sp_size)
    plane, depth = me.plane, me.depth
    tokens, quarter = ctq.shape
    width = quarter * NY
    hidden = wd.shape[0]
    chunk = plane * cap
    half = chunk // 2
    slots = depth * chunk
    distances = [0] + me.dz
    after, before = ((me.sp + 1) % sp_size, me.y), ((me.sp + sp_size - 1) % sp_size, me.y)
    others = [(i, k) for i in range(depth) for k in range(plane) if i + k > 0]
    near = NEAR[depth]
    sent = []
    groups = []

    def columns(y):
        return pl.ds(pl.multiple_of(y * quarter, quarter), quarter)

    def send(src, dst, send_sem, recv_sem, where):
        copy = remote(src, dst, send_sem, recv_sem, where)
        copy.start()
        sent.append(copy)
        return copy

    loads = [
        pltpu.make_async_copy(stream, xall, local.at[0]),
        pltpu.make_async_copy(cotangent.at[:, columns(me.y)], ctq, local.at[1]),
        pltpu.make_async_copy(w_gate, wgu.at[:, pl.ds(0, hidden)], local.at[2]),
        pltpu.make_async_copy(w_up, wgu.at[:, pl.ds(hidden, hidden)], local.at[3]),
        pltpu.make_async_copy(w_down, wd, local.at[4]),
        pltpu.make_async_copy(w_out, wo, local.at[5]),
    ]
    for copy in loads:
        copy.start()

    barrier = pltpu.get_barrier_semaphore()
    partners = [me.at(distances[i], k) for i, k in others] + [me.in_y(y) for y in (me.up, me.across, me.down)]
    for where in partners:
        pl.semaphore_signal(barrier, inc=1, device_id=where, device_id_type=MESH)

    layers = depth // NY
    holder = me.z // layers == me.y
    for k in range(depth):
        where = (k * plane + me.a, me.z // layers)

        @pl.when(jnp.logical_not(jnp.logical_and(holder, me.z == k)))
        def _():
            pl.semaphore_signal(barrier, inc=1, device_id=where, device_id_type=MESH)

    greetings = len(partners) + depth - holder.astype(jnp.int32)

    def iota(shape, dim):
        return lax.broadcasted_iota(jnp.int32, shape, dim)

    square = (tokens, tokens)
    row, col = iota(square, 0), iota(square, 1)
    ids_row = ids[...]
    upright = [
        jnp.broadcast_to(a[k : k + 1, :], (128, tokens)).T
        for a in (ids_row.astype(F32), weights[...])
        for k in range(2)
    ]
    ids_col = [a[:, :1].astype(jnp.int32) for a in upright[:2]]
    weight_col = [a[:, :1] for a in upright[2:]]
    by_col = [
        (iota((tokens, sp_size), 1) == ids_col[k]).astype(F32) for k in range(2)
    ]
    by_row = [
        (iota((sp_size, tokens), 0) == ids_row[k : k + 1, :]).astype(F32) for k in range(2)
    ]
    count_col = jnp.dot(
        (col < row).astype(F32).astype(BF16), (by_col[0] + by_col[1]).astype(BF16),
        preferred_element_type=F32,
    )
    count_row = jnp.dot(
        (by_row[0] + by_row[1]).astype(BF16), (row < col).astype(F32).astype(BF16),
        preferred_element_type=F32,
    )
    place_col, place_row = [], []
    for k in range(2):
        rank = jnp.sum(by_col[k] * count_col, axis=1, keepdims=True).astype(jnp.int32)
        place_col.append(ids_col[k] * cap + rank)
        rank = jnp.sum(by_row[k] * count_row, axis=0, keepdims=True).astype(jnp.int32)
        place_row.append(ids_row[k : k + 1, :] * cap + rank)

    mixed = inner[...].astype(F32) * convin[...].astype(F32)
    ext[pl.ds(8, tokens), :] = mixed

    loads[0].wait()
    loads[1].wait()
    for k in range(2):
        scaled[pl.ds(k * tokens, tokens), :] = (
            weight_col[k] * ctq[...].astype(F32)
        ).astype(BF16)

    def base(i):
        return ((me.z + distances[i]) % depth) * chunk

    def build(i):
        slot = base(i) + iota((chunk, tokens), 0)
        hits = [(slot == place_row[k]).astype(F32) for k in range(2)]
        both = (hits[0] + hits[1]).astype(BF16)
        if i < near:
            picked = jnp.dot(both, xall[...], preferred_element_type=F32).astype(BF16)
            wide_snd[i] = picked.reshape(plane, cap, width)
        else:
            picked = jnp.dot(both, xall[:, columns(me.y)], preferred_element_type=F32).astype(BF16)
            snd[i, :, 0] = picked.reshape(plane, cap, quarter)
        picked = jnp.dot(
            jnp.concatenate(hits, axis=1).astype(BF16), scaled[...], preferred_element_type=F32
        ).astype(BF16)
        snd[i, :, 1] = picked.reshape(plane, cap, quarter)

    def group(i, sends, out_of, send_sem, recv_sem):
        for k in range(plane):
            if i + k > 0:
                src, dst = sends(k)
                remote(src, dst, send_sem, recv_sem, me.at(*out_of(k))).start()

    def whole(ref, send_sem, recv_sem):
        return remote(ref, ref, send_sem, recv_sem, me.in_y(me.up))

    def block(i, k):
        return pl.ds((i * plane + k) * cap, cap)

    def blocks(i):
        return pl.ds(cap, chunk - cap) if i == 0 else pl.ds(i * chunk, chunk)

    def those(ref, i):
        return ref.at[0, pl.ds(0, plane - 1)] if i == 0 else ref.at[i]

    def outward(i):
        return lambda k: (distances[i], k)

    def ship(i):
        if i < near:
            def sends(k):
                target = (me.a + k) % plane
                return snd.at[i, target, 1], rows.at[1, block(i, k), columns(me.y)]
        else:
            def sends(k):
                target = (me.a + k) % plane
                return snd.at[i, target], rows.at[:, block(i, k), columns(me.y)]
        group(i, sends, outward(i), xs.at[i], xr.at[i])
        ref = snd.at[:, :, 1] if i < near else snd
        groups.append(whole(those(ref, i), xs.at[i], xr.at[i]))
        if i == 0:
            rows[1, pl.ds(0, cap), columns(me.y)] = snd[0, me.a, 1]
            rows[0, pl.ds(0, cap), :] = wide_snd[0, me.a]

    def ship_wide(i):
        def sends(k):
            return wide_snd.at[i, (me.a + k) % plane], rows.at[0, block(i, k), :]

        group(i, sends, outward(i), ws.at[i], wr.at[i])
        groups.append(whole(those(wide_snd, i), ws.at[i], wr.at[i]))

    for i in range(depth):
        build(i)
    loads[5].wait()
    pl.semaphore_wait(barrier, greetings)

    direct, relayed = {}, {}

    def round_y(i):
        arrays = 1 if i < near else slice(None)
        whole(rows.at[arrays, blocks(i), columns(me.y)], xs.at[i], xr.at[i]).wait_recv()
        here = rows.at[arrays, pl.ds(i * chunk, chunk), columns(me.y)]
        for j, y in enumerate((me.up, me.down)):
            direct[i, j] = send(here, here, ys.at[i, j], yr.at[i, j], me.in_y(y))

    def relay(i):
        for j, (origin, target) in enumerate(((me.down, me.up), (me.up, me.down))):
            direct[i, j].wait_recv()
            if i < near:
                piece = rows.at[1, pl.ds(i * chunk + j * half, half), columns(origin)]
            else:
                piece = rows.at[j, pl.ds(i * chunk, chunk), columns(origin)]
            relayed[i, j] = send(piece, piece, ys.at[i, 2 + j], yr.at[i, 2 + j], me.in_y(target))

    def finish(i):
        for j in range(2):
            relayed[i, j].wait_recv()
        if i < near:
            whole(rows.at[0, blocks(i), :], ws.at[i], wr.at[i]).wait_recv()

    ready = []

    def expert(g):
        if not ready:
            ready.append(True)
            for k in range(2, 5):
                loads[k].wait()
        here = pl.ds(g * 2 * chunk, 2 * chunk)
        both = jnp.dot(rows[0, here, :], wgu[...], preferred_element_type=F32)
        gate, up = both[:, :hidden], both[:, hidden:]
        d_hidden = lax.dot_general(rows[1, here, :], wd[...], NT, preferred_element_type=F32)
        sig = jax.nn.sigmoid(gate)
        silu = gate * sig
        hid[here, :] = (silu * up).astype(BF16)
        dgu[here, pl.ds(0, hidden)] = (d_hidden * up * sig * (1.0 + gate * (1.0 - sig))).astype(BF16)
        dgu[here, pl.ds(hidden, hidden)] = (d_hidden * silu).astype(BF16)
        part[here, :] = lax.dot_general(
            dgu[here, :], wgu[...], NT, preferred_element_type=F32
        ).astype(BF16)

    got = {}

    def first(i):
        low, high = pl.ds(i * chunk, half), pl.ds(i * chunk + half, half)
        lo, hi = pl.ds(0, half), pl.ds(half, half)
        for j, src, dst, y in (
            (0, part.at[low, columns(me.across)], relays.at[i, 0], me.down),
            (1, part.at[high, columns(me.across)], relays.at[i, 1], me.up),
            (2, part.at[high, columns(me.down)], gotup.at[i, hi], me.down),
            (3, part.at[low, columns(me.up)], gotdown.at[i, lo], me.up),
        ):
            got[i, j] = send(src, dst, rs.at[i, j], rr.at[i, j], me.in_y(y))

    channels = mixer.shape[1]

    def lanes(y):
        return pl.ds(pl.multiple_of(y * channels, channels), channels)

    def to_others(kind, src_of, dst):
        for o in range(1, NY):
            y = (me.y + o) % NY
            exchanged[kind, o] = send(
                src_of(y), dst(o), as_.at[kind, o - 1], ar.at[kind, o - 1], me.in_y(y)
            )

    exchanged = {}

    def share_weights(_):
        exchanged["halo"] = send(
            ext.at[pl.ds(tokens, 8)], ext.at[pl.ds(0, 8)], hs.at[0], hr.at[0], after
        )
        to_others(0, lambda y: wo.at[columns(y), :], lambda o: wall.at[:, lanes(me.y)])
        wall[:, lanes(me.y)] = wo[columns(me.y), :]

    def convolution(_):
        exchanged["halo"].wait_recv()
        ext[pl.ds(0, 8), :] = jnp.where(me.sp == 0, 0.0, ext[pl.ds(0, 8), :])
        conv_out = (
            taps[0:1, :] * ext[pl.ds(6, tokens), :]
            + taps[1:2, :] * ext[pl.ds(7, tokens), :]
            + taps[2:3, :] * ext[pl.ds(8, tokens), :]
        )
        conv[...] = conv_out
        mixer_out = (outer[...].astype(F32) * conv_out).astype(BF16)
        mixer[...] = mixer_out
        mall[:, lanes(me.y)] = mixer_out
        to_others(1, lambda y: mixer, lambda o: mall.at[:, lanes(me.y)])

    jobs = {
        "S": ship, "X": ship_wide, "Y": round_y, "R": relay, "F": finish, "D": expert, "P": first,
        "W": share_weights, "C": convolution,
    }
    for name in ORDERS[depth].split():
        jobs[name[0]](int(name[1:]))

    def second(i):
        low, high = pl.ds(i * chunk, half), pl.ds(i * chunk + half, half)
        lo, hi = pl.ds(0, half), pl.ds(half, half)
        for j, mine, y, dst in (
            (0, low, me.down, gotup.at[i, lo]),
            (1, high, me.up, gotdown.at[i, hi]),
        ):
            got[i, j].wait_recv()
            sums[i, j] = (
                part[mine, columns(y)].astype(F32) + relays[i, j].astype(F32)
            ).astype(BF16)
            got[i, 4 + j] = send(sums.at[i, j], dst, rs.at[i, 4 + j], rr.at[i, 4 + j], me.in_y(y))

    def third(i):
        for j in range(2, 6):
            got[i, j].wait_recv()
        total = (
            part[pl.ds(i * chunk, chunk), columns(me.y)].astype(F32)
            + gotup[i].astype(F32)
            + gotdown[i].astype(F32)
        ).astype(BF16)
        share[i] = total.reshape(plane, cap, quarter)
        if i == 0:
            ret[0, me.a] = share[0, 0]

        def sends(k):
            return share.at[i, k], ret.at[i, me.a]

        group(i, sends, lambda k: (depth - distances[i], plane - k), ps.at[i], pr.at[i])
        groups.append(whole(those(share, i), ps.at[i], pr.at[i]))

    def fourth(i):
        whole(those(ret, i), ps.at[i], pr.at[i]).wait_recv()
        slot = base(i) + iota((tokens, chunk), 1)
        hit = ((slot == place_col[0]) | (slot == place_col[1])).astype(F32).astype(BF16)
        moe[...] += jnp.dot(hit, ret[i].reshape(chunk, quarter), preferred_element_type=F32)

    tiles = depth
    wide = width // tiles

    def weight_grads(t):
        cols = pl.ds(t * wide, wide)
        both = lax.dot_general(rows[0, :, cols], dgu[...], TN, preferred_element_type=F32)
        g_gate[0, cols, :] = both[:, :hidden].astype(BF16)
        g_up[0, cols, :] = both[:, hidden:].astype(BF16)
        g_down[0, :, cols] = lax.dot_general(
            hid[...], rows[1, :, cols], TN, preferred_element_type=F32
        ).astype(BF16)

    order = RETURNS[depth]
    moe[...] = ctq[...].astype(F32)
    early = 2
    for step in range(depth + 1):
        if step + 2 < depth and step + 2 >= early:
            first(order[step + 2])
        if step < depth:
            second(order[step])
        if step >= 1:
            third(order[step - 1])
        if step < tiles:
            weight_grads(step)
    for k in range(depth):
        fourth(order[k])

    for o in range(1, NY):
        exchanged[1, o].wait_recv()
        exchanged[0, o].wait_recv()
    stream_grad = moe[...].astype(BF16)
    core = me.a % 2
    across_x = me.a // 2
    chips = plane // 2
    gp[...] = (
        lax.dot_general(stream_grad, mall[...], TN, preferred_element_type=F32)
        .astype(BF16)
        .reshape(gp.shape)
    )
    between = send(
        gp.at[:, :, 1 - core], cbuf, cs.at[0], cr.at[0],
        (me.z * plane + across_x * 2 + 1 - core, me.y),
    )
    for o in range(1, NY):
        y = (me.y + o) % NY
        dsend[o - 1] = jnp.dot(
            stream_grad, wall[:, lanes(y)], preferred_element_type=F32
        ).astype(BF16)
    to_others(2, lambda y: dsend.at[(y - me.y + NY) % NY - 1], lambda o: dgot.at[o - 1])
    d_mixer = jnp.dot(stream_grad, wall[:, lanes(me.y)], preferred_element_type=F32)

    between.wait_recv()
    summed = gp[:, :, core].astype(F32) + cbuf[...].astype(F32)
    hx[...] = summed.astype(BF16)
    over_x = []
    for d in range(1, chips):
        target = (across_x + d) % chips
        over_x.append(
            send(
                hx.at[:, target], xbuf.at[d - 1], gs.at[d - 1], gr.at[d - 1],
                (me.z * plane + target * 2 + core, me.y),
            )
        )

    for o in range(1, NY):
        exchanged[2, o].wait_recv()
        d_mixer += dgot[o - 1].astype(F32)
    dext[pl.ds(0, tokens), :] = d_mixer * outer[...].astype(F32)
    trail = send(dext.at[pl.ds(0, 8)], dext.at[pl.ds(tokens, 8)], hs.at[1], hr.at[1], before)
    g_outer[...] = d_mixer * conv[...]

    summed = hx[:, across_x].astype(F32)
    for d in range(1, chips):
        over_x[d - 1].wait_recv()
        summed += xbuf[d - 1].astype(F32)
    to_owner = []
    for k in range(layers):
        for y in range(NY):
            hz[k, y] = summed[k, :, y * channels : (y + 1) * channels].astype(BF16)
            owner = layers * me.y + k
            mine = jnp.logical_and(owner == me.z, me.y == y)
            copy = remote(
                hz.at[k, y], zsum.at[me.z], ts.at[k, y], tr.at[me.z], (owner * plane + me.a, y)
            )
            to_owner.append((mine, copy))

            @pl.when(mine)
            def _():
                zsum[me.z] = hz[k, y]

            @pl.when(jnp.logical_not(mine))
            def _():
                copy.start()

    trail.wait_recv()
    dext[pl.ds(tokens, 8), :] = jnp.where(me.sp == sp_size - 1, 0.0, dext[pl.ds(tokens, 8), :])
    d_mixed = (
        taps[2:3, :] * dext[pl.ds(0, tokens), :]
        + taps[1:2, :] * dext[pl.ds(1, tokens), :]
        + taps[0:1, :] * dext[pl.ds(2, tokens), :]
    )
    g_inner[...] = d_mixed * convin[...].astype(F32)
    g_convin[...] = d_mixed * inner[...].astype(F32)

    for k in range(depth):
        @pl.when(jnp.logical_not(jnp.logical_and(holder, me.z == k)))
        def _():
            remote(zsum.at[k], zsum.at[k], ts.at[0, 0], tr.at[k], me.in_y(me.up)).wait_recv()

    total = zsum[0].astype(F32)
    for k in range(1, depth):
        total += zsum[k].astype(F32)
    g_out[...] = total
    for copy in sent + groups:
        copy.wait_send()
    for mine, copy in to_owner:
        @pl.when(jnp.logical_not(mine))
        def _():
            copy.wait_send()


def shards(
    out_cotangent,
    stream,
    route_ids,
    route_weights,
    gate_proj,
    up_proj,
    down_proj,
    outer_gate,
    inner_gate,
    conv_input,
    conv_taps,
    out_proj,
):
    sp = lax.axis_size("sp")
    plane = plane_size(sp)
    depth = sp // plane
    tokens, width = stream.shape
    cap = 4 * tokens // sp
    chunk = plane * cap
    slots = depth * chunk
    quarter = width // NY
    hidden = gate_proj.shape[2]
    channels = outer_gate.shape[1]
    layers = depth // NY
    chips = plane // 2
    near = NEAR[depth]
    block = width // sp
    vmem = pl.BlockSpec(memory_space=pltpu.VMEM)
    hbm = pl.BlockSpec(memory_space=pl.ANY)

    def dma(*shape):
        return pltpu.SemaphoreType.DMA(shape)

    def bf16(*shape):
        return pltpu.VMEM(shape, BF16)

    def f32(*shape):
        return pltpu.VMEM(shape, F32)

    shapes = (
        ((1, width, hidden), BF16),
        ((1, width, hidden), BF16),
        ((1, hidden, width), BF16),
        ((block, channels), F32),
        ((tokens, channels), F32),
        ((tokens, channels), F32),
        ((tokens, channels), F32),
    )
    return pl.pallas_call(
        functools.partial(layer_kernel, sp, cap),
        name="layer",
        out_shape=tuple(pltpu.VMEM(*s) for s in shapes),
        in_specs=[vmem] * 6 + [hbm] * 6,
        out_specs=(vmem,) * 7,
        scratch_shapes=[
            bf16(tokens, width),
            bf16(tokens, quarter),
            bf16(2 * tokens, quarter),
            bf16(width, 2 * hidden),
            bf16(hidden, width),
            bf16(width, channels),
            bf16(depth, plane, 2, cap, quarter),
            bf16(near, plane, cap, width),
            bf16(2, slots, width),
            bf16(slots, hidden),
            bf16(slots, 2 * hidden),
            bf16(slots, width),
            bf16(depth, chunk, quarter),
            bf16(depth, chunk, quarter),
            bf16(depth, 2, chunk // 2, quarter),
            bf16(depth, 2, chunk // 2, quarter),
            bf16(depth, plane, cap, quarter),
            bf16(depth, plane, cap, quarter),
            f32(tokens, quarter),
            bf16(quarter, NY * channels),
            bf16(tokens, NY * channels),
            bf16(NY - 1, tokens, channels),
            bf16(NY - 1, tokens, channels),
            f32(tokens + 8, channels),
            f32(tokens + 8, channels),
            bf16(tokens, channels),
            f32(tokens, channels),
            bf16(layers, chips, 2, block, NY * channels),
            bf16(layers, chips, block, NY * channels),
            bf16(layers, chips, block, NY * channels),
            bf16(max(chips - 1, 1), layers, block, NY * channels),
            bf16(layers, NY, block, channels),
            bf16(depth, block, channels),
            dma(6),
            dma(depth),
            dma(depth),
            dma(near),
            dma(near),
            dma(depth, 4),
            dma(depth, 4),
            dma(depth, 6),
            dma(depth, 6),
            dma(depth),
            dma(depth),
            dma(3, NY - 1),
            dma(3, NY - 1),
            dma(2),
            dma(2),
            dma(1),
            dma(1),
            dma(max(chips - 1, 1)),
            dma(max(chips - 1, 1)),
            dma(layers, NY),
            dma(depth),
        ],
        compiler_params=pltpu.CompilerParams(
            collective_id=0, has_side_effects=True, vmem_limit_bytes=60 * 1024 * 1024
        ),
    )(
        route_ids.T, route_weights.T, outer_gate, inner_gate, conv_input, conv_taps,
        out_cotangent, stream, gate_proj[0], up_proj[0], down_proj[0], out_proj,
    )


def solution(mesh):
    placed = (
        P("sp", None),
        P("sp", None),
        P("sp", None),
        P("sp", None),
        P("sp", None, "tp"),
        P("sp", None, "tp"),
        P("sp", "tp", None),
        P("sp", "tp"),
        P("sp", "tp"),
        P("sp", "tp"),
        P(None, "tp"),
        P(None, "tp"),
    )
    return jax.shard_map(
        shards,
        mesh=mesh,
        in_specs=placed,
        out_specs=(
            P("sp", None, "tp"),
            P("sp", None, "tp"),
            P("sp", "tp", None),
            P("sp", "tp"),
            P("sp", "tp"),
            P("sp", "tp"),
            P("sp", "tp"),
        ),
        check_vma=False,
    )
```

```python
import functools

import jax
import jax.numpy as jnp
from jax import lax
from jax.experimental import pallas as pl
from jax.experimental.pallas import tpu as pltpu
from jax.sharding import PartitionSpec as P

MESH = pl.DeviceIdType.MESH
F32 = jnp.float32
BF16 = jnp.bfloat16
NY = 4


def plane_size(sp):
    return sp // 8


def offsets(n):
    out = []
    for d in range(1, n // 2 + 1):
        out.append(d)
        if n - d != d:
            out.append(n - d)
    return out


def remote(src, dst, send, recv, where):
    return pltpu.make_async_remote_copy(
        src_ref=src, dst_ref=dst, send_sem=send, recv_sem=recv, device_id=where, device_id_type=MESH
    )


class Place:
    def __init__(self, sp_size):
        self.plane = plane_size(sp_size)
        self.depth = sp_size // self.plane
        self.sp = lax.axis_index("sp")
        self.y = lax.axis_index("tp")
        self.z = self.sp // self.plane
        self.a = self.sp % self.plane
        self.up = (self.y + 1) % NY
        self.down = (self.y + NY - 1) % NY
        self.across = (self.y + 2) % NY
        self.dz = offsets(self.depth)
        self.da = list(range(1, self.plane))

    def at(self, d, k):
        plane = self.plane
        return (((self.z + d) % self.depth) * plane + (self.a + k) % plane, self.y)

    def in_y(self, y):
        return (self.sp, y)


ORDERS = {
    8: "S1 S2 W0 S3 S4 S5 S6 Y1 Y2 S7 C0 R1 X0 R2 X1 X2 Y3 Y4 R3 R4 Y5 Y6 R5 Y7 R6 R7 F4 F5 D2 P5 P4 "
    "F6 F7 D3 F2 F3 D1 F0 F1 D0",
}
NEAR = {8: 3}
RETURNS = {8: (5, 4, 7, 6, 3, 2, 1, 0)}
NT = (((1,), (1,)), ((), ()))
TN = (((0,), (0,)), ((), ()))


def layer_kernel(
    sp_size,
    cap,
    ids, weights, outer, inner, convin, taps,
    cotangent, stream, w_gate, w_up, w_down, w_out,
    g_gate, g_up, g_down, g_out, g_outer, g_inner, g_convin,
    xall, call, scaled, wgu, wd, wo,
    snd, full_snd, wide_snd, rows, hid, dgu, part,
    gotup, gotdown, relays, sums, share, ret, moe, wall, mall, dsend, dgot,
    ext, dext, mixer, conv, gp, cbuf, hx, xbuf, hz, zsum,
    local, xs, xr, ws, wr, ys, yr, rs, rr, ps, pr, as_, ar, hs, hr, cs, cr, gs, gr, ts, tr,
):
    me = Place(sp_size)
    plane, depth = me.plane, me.depth
    tokens, width = call.shape
    quarter = width // NY
    hidden = wd.shape[0]
    chunk = plane * cap
    half = chunk // 2
    slots = depth * chunk
    distances = [0] + me.dz
    after, before = ((me.sp + 1) % sp_size, me.y), ((me.sp + sp_size - 1) % sp_size, me.y)
    others = [(i, k) for i in range(depth) for k in range(plane) if i + k > 0]
    near = NEAR[depth]
    sent = []
    groups = []

    def columns(y):
        return pl.ds(pl.multiple_of(y * quarter, quarter), quarter)

    def send(src, dst, send_sem, recv_sem, where):
        copy = remote(src, dst, send_sem, recv_sem, where)
        copy.start()
        sent.append(copy)
        return copy

    loads = [
        pltpu.make_async_copy(stream, xall, local.at[0]),
        pltpu.make_async_copy(cotangent, call, local.at[1]),
        pltpu.make_async_copy(w_gate, wgu.at[:, pl.ds(0, hidden)], local.at[2]),
        pltpu.make_async_copy(w_up, wgu.at[:, pl.ds(hidden, hidden)], local.at[3]),
        pltpu.make_async_copy(w_down, wd, local.at[4]),
        pltpu.make_async_copy(w_out, wo, local.at[5]),
    ]
    for copy in loads:
        copy.start()

    barrier = pltpu.get_barrier_semaphore()
    partners = [me.at(distances[i], k) for i, k in others] + [me.in_y(y) for y in (me.up, me.across, me.down)]
    for where in partners:
        pl.semaphore_signal(barrier, inc=1, device_id=where, device_id_type=MESH)

    layers = depth // NY
    holder = me.z // layers == me.y
    for k in range(depth):
        where = (k * plane + me.a, me.z // layers)

        @pl.when(jnp.logical_not(jnp.logical_and(holder, me.z == k)))
        def _():
            pl.semaphore_signal(barrier, inc=1, device_id=where, device_id_type=MESH)

    greetings = len(partners) + depth - holder.astype(jnp.int32)

    def iota(shape, dim):
        return lax.broadcasted_iota(jnp.int32, shape, dim)

    square = (tokens, tokens)
    row, col = iota(square, 0), iota(square, 1)
    ids_row = ids[...]
    upright = [
        jnp.broadcast_to(a[k : k + 1, :], (128, tokens)).T
        for a in (ids_row.astype(F32), weights[...])
        for k in range(2)
    ]
    ids_col = [a[:, :1].astype(jnp.int32) for a in upright[:2]]
    weight_col = [a[:, :1] for a in upright[2:]]
    by_col = [
        (iota((tokens, sp_size), 1) == ids_col[k]).astype(F32) for k in range(2)
    ]
    by_row = [
        (iota((sp_size, tokens), 0) == ids_row[k : k + 1, :]).astype(F32) for k in range(2)
    ]
    count_col = jnp.dot(
        (col < row).astype(F32).astype(BF16), (by_col[0] + by_col[1]).astype(BF16),
        preferred_element_type=F32,
    )
    count_row = jnp.dot(
        (by_row[0] + by_row[1]).astype(BF16), (row < col).astype(F32).astype(BF16),
        preferred_element_type=F32,
    )
    place_col, place_row = [], []
    for k in range(2):
        rank = jnp.sum(by_col[k] * count_col, axis=1, keepdims=True).astype(jnp.int32)
        place_col.append(ids_col[k] * cap + rank)
        rank = jnp.sum(by_row[k] * count_row, axis=0, keepdims=True).astype(jnp.int32)
        place_row.append(ids_row[k : k + 1, :] * cap + rank)

    mixed = inner[...].astype(F32) * convin[...].astype(F32)
    ext[pl.ds(8, tokens), :] = mixed

    loads[0].wait()
    loads[1].wait()
    for k in range(2):
        scaled[pl.ds(k * tokens, tokens), :] = (
            weight_col[k] * call[...].astype(F32)
        ).astype(BF16)

    def base(i):
        return ((me.z + distances[i]) % depth) * chunk

    def build(i):
        slot = base(i) + iota((chunk, tokens), 0)
        hits = [(slot == place_row[k]).astype(F32) for k in range(2)]
        both = (hits[0] + hits[1]).astype(BF16)
        apart = jnp.concatenate(hits, axis=1).astype(BF16)
        here = columns(me.y)
        if i == 0:
            picked = jnp.dot(both, xall[...], preferred_element_type=F32).astype(BF16)
            full_snd[:, 0] = picked.reshape(plane, cap, width)
            picked = jnp.dot(apart, scaled[...], preferred_element_type=F32).astype(BF16)
            full_snd[:, 1] = picked.reshape(plane, cap, width)
            return
        if i < near:
            picked = jnp.dot(both, xall[...], preferred_element_type=F32).astype(BF16)
            wide_snd[i - 1] = picked.reshape(plane, cap, width)
        else:
            picked = jnp.dot(both, xall[:, here], preferred_element_type=F32).astype(BF16)
            snd[i, :, 0] = picked.reshape(plane, cap, quarter)
        picked = jnp.dot(apart, scaled[:, here], preferred_element_type=F32).astype(BF16)
        snd[i, :, 1] = picked.reshape(plane, cap, quarter)

    def group(i, sends, out_of, send_sem, recv_sem):
        for k in range(plane):
            if i + k > 0:
                src, dst = sends(k)
                remote(src, dst, send_sem, recv_sem, me.at(*out_of(k))).start()

    def whole(ref, send_sem, recv_sem):
        return remote(ref, ref, send_sem, recv_sem, me.in_y(me.up))

    def block(i, k):
        return pl.ds((i * plane + k) * cap, cap)

    def blocks(i):
        return pl.ds(cap, chunk - cap) if i == 0 else pl.ds(i * chunk, chunk)

    def those(ref, i):
        return ref.at[0, pl.ds(0, plane - 1)] if i == 0 else ref.at[i]

    def outward(i):
        return lambda k: (distances[i], k)

    def ship(i):
        if i < near:
            def sends(k):
                target = (me.a + k) % plane
                return snd.at[i, target, 1], rows.at[1, block(i, k), columns(me.y)]
        else:
            def sends(k):
                target = (me.a + k) % plane
                return snd.at[i, target], rows.at[:, block(i, k), columns(me.y)]
        group(i, sends, outward(i), xs.at[i], xr.at[i])
        ref = snd.at[:, :, 1] if i < near else snd
        groups.append(whole(those(ref, i), xs.at[i], xr.at[i]))

    def ship_wide(i):
        def sends(k):
            target = (me.a + k) % plane
            if i == 0:
                return full_snd.at[target], rows.at[:, block(i, k), :]
            return wide_snd.at[i - 1, target], rows.at[0, block(i, k), :]

        group(i, sends, outward(i), ws.at[i], wr.at[i])
        sent_refs = full_snd.at[pl.ds(0, plane - 1)] if i == 0 else wide_snd.at[i - 1]
        groups.append(whole(sent_refs, ws.at[i], wr.at[i]))
        if i == 0:
            rows[:, pl.ds(0, cap), :] = full_snd[me.a]

    for i in range(depth):
        build(i)
    loads[5].wait()
    pl.semaphore_wait(barrier, greetings)

    direct, relayed = {}, {}

    def round_y(i):
        arrays = 1 if i < near else slice(None)
        whole(rows.at[arrays, blocks(i), columns(me.y)], xs.at[i], xr.at[i]).wait_recv()
        here = rows.at[arrays, pl.ds(i * chunk, chunk), columns(me.y)]
        for j, y in enumerate((me.up, me.down)):
            direct[i, j] = send(here, here, ys.at[i, j], yr.at[i, j], me.in_y(y))

    def relay(i):
        for j, (origin, target) in enumerate(((me.down, me.up), (me.up, me.down))):
            direct[i, j].wait_recv()
            if i < near:
                piece = rows.at[1, pl.ds(i * chunk + j * half, half), columns(origin)]
            else:
                piece = rows.at[j, pl.ds(i * chunk, chunk), columns(origin)]
            relayed[i, j] = send(piece, piece, ys.at[i, 2 + j], yr.at[i, 2 + j], me.in_y(target))

    def finish(i):
        if i > 0:
            for j in range(2):
                relayed[i, j].wait_recv()
        if i < near:
            arrays = slice(None) if i == 0 else 0
            whole(rows.at[arrays, blocks(i), :], ws.at[i], wr.at[i]).wait_recv()

    ready = []

    def expert(g):
        if not ready:
            ready.append(True)
            for k in range(2, 5):
                loads[k].wait()
        here = pl.ds(g * 2 * chunk, 2 * chunk)
        both = jnp.dot(rows[0, here, :], wgu[...], preferred_element_type=F32)
        gate, up = both[:, :hidden], both[:, hidden:]
        d_hidden = lax.dot_general(rows[1, here, :], wd[...], NT, preferred_element_type=F32)
        sig = jax.nn.sigmoid(gate)
        silu = gate * sig
        hid[here, :] = (silu * up).astype(BF16)
        dgu[here, pl.ds(0, hidden)] = (d_hidden * up * sig * (1.0 + gate * (1.0 - sig))).astype(BF16)
        dgu[here, pl.ds(hidden, hidden)] = (d_hidden * silu).astype(BF16)
        part[here, :] = lax.dot_general(
            dgu[here, :], wgu[...], NT, preferred_element_type=F32
        ).astype(BF16)

    got = {}

    def first(i):
        low, high = pl.ds(i * chunk, half), pl.ds(i * chunk + half, half)
        lo, hi = pl.ds(0, half), pl.ds(half, half)
        for j, src, dst, y in (
            (0, part.at[low, columns(me.across)], relays.at[i, 0], me.down),
            (1, part.at[high, columns(me.across)], relays.at[i, 1], me.up),
            (2, part.at[high, columns(me.down)], gotup.at[i, hi], me.down),
            (3, part.at[low, columns(me.up)], gotdown.at[i, lo], me.up),
        ):
            got[i, j] = send(src, dst, rs.at[i, j], rr.at[i, j], me.in_y(y))

    channels = mixer.shape[1]

    def lanes(y):
        return pl.ds(pl.multiple_of(y * channels, channels), channels)

    def to_others(kind, src_of, dst):
        for o in range(1, NY):
            y = (me.y + o) % NY
            exchanged[kind, o] = send(
                src_of(y), dst(o), as_.at[kind, o - 1], ar.at[kind, o - 1], me.in_y(y)
            )

    exchanged = {}

    def share_weights(_):
        exchanged["halo"] = send(
            ext.at[pl.ds(tokens, 8)], ext.at[pl.ds(0, 8)], hs.at[0], hr.at[0], after
        )
        to_others(0, lambda y: wo.at[columns(y), :], lambda o: wall.at[:, lanes(me.y)])
        wall[:, lanes(me.y)] = wo[columns(me.y), :]

    def convolution(_):
        exchanged["halo"].wait_recv()
        ext[pl.ds(0, 8), :] = jnp.where(me.sp == 0, 0.0, ext[pl.ds(0, 8), :])
        conv_out = (
            taps[0:1, :] * ext[pl.ds(6, tokens), :]
            + taps[1:2, :] * ext[pl.ds(7, tokens), :]
            + taps[2:3, :] * ext[pl.ds(8, tokens), :]
        )
        conv[...] = conv_out
        mixer_out = (outer[...].astype(F32) * conv_out).astype(BF16)
        mixer[...] = mixer_out
        mall[:, lanes(me.y)] = mixer_out
        to_others(1, lambda y: mixer, lambda o: mall.at[:, lanes(me.y)])

    jobs = {
        "S": ship, "X": ship_wide, "Y": round_y, "R": relay, "F": finish, "D": expert, "P": first,
        "W": share_weights, "C": convolution,
    }
    for name in ORDERS[depth].split():
        jobs[name[0]](int(name[1:]))

    def second(i):
        low, high = pl.ds(i * chunk, half), pl.ds(i * chunk + half, half)
        lo, hi = pl.ds(0, half), pl.ds(half, half)
        for j, mine, y, dst in (
            (0, low, me.down, gotup.at[i, lo]),
            (1, high, me.up, gotdown.at[i, hi]),
        ):
            got[i, j].wait_recv()
            sums[i, j] = (
                part[mine, columns(y)].astype(F32) + relays[i, j].astype(F32)
            ).astype(BF16)
            got[i, 4 + j] = send(sums.at[i, j], dst, rs.at[i, 4 + j], rr.at[i, 4 + j], me.in_y(y))

    def third(i):
        for j in range(2, 6):
            got[i, j].wait_recv()
        total = (
            part[pl.ds(i * chunk, chunk), columns(me.y)].astype(F32)
            + gotup[i].astype(F32)
            + gotdown[i].astype(F32)
        ).astype(BF16)
        share[i] = total.reshape(plane, cap, quarter)
        if i == 0:
            ret[0, me.a] = share[0, 0]

        def sends(k):
            return share.at[i, k], ret.at[i, me.a]

        group(i, sends, lambda k: (depth - distances[i], plane - k), ps.at[i], pr.at[i])
        groups.append(whole(those(share, i), ps.at[i], pr.at[i]))

    def fourth(i):
        whole(those(ret, i), ps.at[i], pr.at[i]).wait_recv()
        slot = base(i) + iota((tokens, chunk), 1)
        hit = ((slot == place_col[0]) | (slot == place_col[1])).astype(F32).astype(BF16)
        moe[...] += jnp.dot(hit, ret[i].reshape(chunk, quarter), preferred_element_type=F32)

    tiles = depth
    wide = width // tiles

    def weight_grads(t):
        cols = pl.ds(t * wide, wide)
        both = lax.dot_general(rows[0, :, cols], dgu[...], TN, preferred_element_type=F32)
        g_gate[0, cols, :] = both[:, :hidden].astype(BF16)
        g_up[0, cols, :] = both[:, hidden:].astype(BF16)
        g_down[0, :, cols] = lax.dot_general(
            hid[...], rows[1, :, cols], TN, preferred_element_type=F32
        ).astype(BF16)

    order = RETURNS[depth]
    moe[...] = call[:, columns(me.y)].astype(F32)
    early = 2
    for step in range(depth + 1):
        if step + 2 < depth and step + 2 >= early:
            first(order[step + 2])
        if step < depth:
            second(order[step])
        if step >= 1:
            third(order[step - 1])
        if step < tiles:
            weight_grads(step)
    for k in range(depth):
        fourth(order[k])

    for o in range(1, NY):
        exchanged[1, o].wait_recv()
        exchanged[0, o].wait_recv()
    stream_grad = moe[...].astype(BF16)
    core = me.a % 2
    across_x = me.a // 2
    chips = plane // 2
    gp[...] = (
        lax.dot_general(stream_grad, mall[...], TN, preferred_element_type=F32)
        .astype(BF16)
        .reshape(gp.shape)
    )
    between = send(
        gp.at[:, :, 1 - core], cbuf, cs.at[0], cr.at[0],
        (me.z * plane + across_x * 2 + 1 - core, me.y),
    )
    for o in range(1, NY):
        y = (me.y + o) % NY
        dsend[o - 1] = jnp.dot(
            stream_grad, wall[:, lanes(y)], preferred_element_type=F32
        ).astype(BF16)
    to_others(2, lambda y: dsend.at[(y - me.y + NY) % NY - 1], lambda o: dgot.at[o - 1])
    d_mixer = jnp.dot(stream_grad, wall[:, lanes(me.y)], preferred_element_type=F32)

    between.wait_recv()
    summed = gp[:, :, core].astype(F32) + cbuf[...].astype(F32)
    hx[...] = summed.astype(BF16)
    over_x = []
    for d in range(1, chips):
        target = (across_x + d) % chips
        over_x.append(
            send(
                hx.at[:, target], xbuf.at[d - 1], gs.at[d - 1], gr.at[d - 1],
                (me.z * plane + target * 2 + core, me.y),
            )
        )

    for o in range(1, NY):
        exchanged[2, o].wait_recv()
        d_mixer += dgot[o - 1].astype(F32)
    dext[pl.ds(0, tokens), :] = d_mixer * outer[...].astype(F32)
    trail = send(dext.at[pl.ds(0, 8)], dext.at[pl.ds(tokens, 8)], hs.at[1], hr.at[1], before)
    g_outer[...] = d_mixer * conv[...]

    summed = hx[:, across_x].astype(F32)
    for d in range(1, chips):
        over_x[d - 1].wait_recv()
        summed += xbuf[d - 1].astype(F32)
    to_owner = []
    for k in range(layers):
        for y in range(NY):
            hz[k, y] = summed[k, :, y * channels : (y + 1) * channels].astype(BF16)
            owner = layers * me.y + k
            mine = jnp.logical_and(owner == me.z, me.y == y)
            copy = remote(
                hz.at[k, y], zsum.at[me.z], ts.at[k, y], tr.at[me.z], (owner * plane + me.a, y)
            )
            to_owner.append((mine, copy))

            @pl.when(mine)
            def _():
                zsum[me.z] = hz[k, y]

            @pl.when(jnp.logical_not(mine))
            def _():
                copy.start()

    trail.wait_recv()
    dext[pl.ds(tokens, 8), :] = jnp.where(me.sp == sp_size - 1, 0.0, dext[pl.ds(tokens, 8), :])
    d_mixed = (
        taps[2:3, :] * dext[pl.ds(0, tokens), :]
        + taps[1:2, :] * dext[pl.ds(1, tokens), :]
        + taps[0:1, :] * dext[pl.ds(2, tokens), :]
    )
    g_inner[...] = d_mixed * convin[...].astype(F32)
    g_convin[...] = d_mixed * inner[...].astype(F32)

    for k in range(depth):
        @pl.when(jnp.logical_not(jnp.logical_and(holder, me.z == k)))
        def _():
            remote(zsum.at[k], zsum.at[k], ts.at[0, 0], tr.at[k], me.in_y(me.up)).wait_recv()

    total = zsum[0].astype(F32)
    for k in range(1, depth):
        total += zsum[k].astype(F32)
    g_out[...] = total
    for copy in sent + groups:
        copy.wait_send()
    for mine, copy in to_owner:
        @pl.when(jnp.logical_not(mine))
        def _():
            copy.wait_send()


def shards(
    out_cotangent,
    stream,
    route_ids,
    route_weights,
    gate_proj,
    up_proj,
    down_proj,
    outer_gate,
    inner_gate,
    conv_input,
    conv_taps,
    out_proj,
):
    sp = lax.axis_size("sp")
    plane = plane_size(sp)
    depth = sp // plane
    tokens, width = stream.shape
    cap = 4 * tokens // sp
    chunk = plane * cap
    slots = depth * chunk
    quarter = width // NY
    hidden = gate_proj.shape[2]
    channels = outer_gate.shape[1]
    layers = depth // NY
    chips = plane // 2
    near = NEAR[depth]
    block = width // sp
    vmem = pl.BlockSpec(memory_space=pltpu.VMEM)
    hbm = pl.BlockSpec(memory_space=pl.ANY)

    def dma(*shape):
        return pltpu.SemaphoreType.DMA(shape)

    def bf16(*shape):
        return pltpu.VMEM(shape, BF16)

    def f32(*shape):
        return pltpu.VMEM(shape, F32)

    shapes = (
        ((1, width, hidden), BF16),
        ((1, width, hidden), BF16),
        ((1, hidden, width), BF16),
        ((block, channels), F32),
        ((tokens, channels), F32),
        ((tokens, channels), F32),
        ((tokens, channels), F32),
    )
    return pl.pallas_call(
        functools.partial(layer_kernel, sp, cap),
        name="layer",
        out_shape=tuple(pltpu.VMEM(*s) for s in shapes),
        in_specs=[vmem] * 6 + [hbm] * 6,
        out_specs=(vmem,) * 7,
        scratch_shapes=[
            bf16(tokens, width),
            bf16(tokens, width),
            bf16(2 * tokens, width),
            bf16(width, 2 * hidden),
            bf16(hidden, width),
            bf16(width, channels),
            bf16(depth, plane, 2, cap, quarter),
            bf16(plane, 2, cap, width),
            bf16(max(near - 1, 1), plane, cap, width),
            bf16(2, slots, width),
            bf16(slots, hidden),
            bf16(slots, 2 * hidden),
            bf16(slots, width),
            bf16(depth, chunk, quarter),
            bf16(depth, chunk, quarter),
            bf16(depth, 2, chunk // 2, quarter),
            bf16(depth, 2, chunk // 2, quarter),
            bf16(depth, plane, cap, quarter),
            bf16(depth, plane, cap, quarter),
            f32(tokens, quarter),
            bf16(quarter, NY * channels),
            bf16(tokens, NY * channels),
            bf16(NY - 1, tokens, channels),
            bf16(NY - 1, tokens, channels),
            f32(tokens + 8, channels),
            f32(tokens + 8, channels),
            bf16(tokens, channels),
            f32(tokens, channels),
            bf16(layers, chips, 2, block, NY * channels),
            bf16(layers, chips, block, NY * channels),
            bf16(layers, chips, block, NY * channels),
            bf16(max(chips - 1, 1), layers, block, NY * channels),
            bf16(layers, NY, block, channels),
            bf16(depth, block, channels),
            dma(6),
            dma(depth),
            dma(depth),
            dma(near),
            dma(near),
            dma(depth, 4),
            dma(depth, 4),
            dma(depth, 6),
            dma(depth, 6),
            dma(depth),
            dma(depth),
            dma(3, NY - 1),
            dma(3, NY - 1),
            dma(2),
            dma(2),
            dma(1),
            dma(1),
            dma(max(chips - 1, 1)),
            dma(max(chips - 1, 1)),
            dma(layers, NY),
            dma(depth),
        ],
        compiler_params=pltpu.CompilerParams(
            collective_id=0, has_side_effects=True, vmem_limit_bytes=60 * 1024 * 1024
        ),
    )(
        route_ids.T, route_weights.T, outer_gate, inner_gate, conv_input, conv_taps,
        out_cotangent, stream, gate_proj[0], up_proj[0], down_proj[0], out_proj,
    )


def solution(mesh):
    placed = (
        P("sp", None),
        P("sp", None),
        P("sp", None),
        P("sp", None),
        P("sp", None, "tp"),
        P("sp", None, "tp"),
        P("sp", "tp", None),
        P("sp", "tp"),
        P("sp", "tp"),
        P("sp", "tp"),
        P(None, "tp"),
        P(None, "tp"),
    )
    return jax.shard_map(
        shards,
        mesh=mesh,
        in_specs=placed,
        out_specs=(
            P("sp", None, "tp"),
            P("sp", None, "tp"),
            P("sp", "tp", None),
            P("sp", "tp"),
            P("sp", "tp"),
            P("sp", "tp"),
            P("sp", "tp"),
        ),
        check_vma=False,
    )
```

```python
import functools

import jax
import jax.numpy as jnp
from jax import lax
from jax.experimental import pallas as pl
from jax.experimental.pallas import tpu as pltpu
from jax.sharding import PartitionSpec as P

MESH = pl.DeviceIdType.MESH
F32 = jnp.float32
BF16 = jnp.bfloat16
NY = 4


def plane_size(sp):
    return sp // 8


def offsets(n):
    out = []
    for d in range(1, n // 2 + 1):
        out.append(d)
        if n - d != d:
            out.append(n - d)
    return out


def remote(src, dst, send, recv, where):
    return pltpu.make_async_remote_copy(
        src_ref=src, dst_ref=dst, send_sem=send, recv_sem=recv, device_id=where, device_id_type=MESH
    )


class Place:
    def __init__(self, sp_size):
        self.plane = plane_size(sp_size)
        self.depth = sp_size // self.plane
        self.sp = lax.axis_index("sp")
        self.y = lax.axis_index("tp")
        self.z = self.sp // self.plane
        self.a = self.sp % self.plane
        self.up = (self.y + 1) % NY
        self.down = (self.y + NY - 1) % NY
        self.across = (self.y + 2) % NY
        self.dz = offsets(self.depth)
        self.da = list(range(1, self.plane))

    def at(self, d, k):
        plane = self.plane
        return (((self.z + d) % self.depth) * plane + (self.a + k) % plane, self.y)

    def in_y(self, y):
        return (self.sp, y)


ORDERS = {
    8: "S1 S2 W0 S3 S4 S5 S6 Y1 Y2 S7 C0 R1 X0 R2 X1 X2 Y3 Y4 R3 R4 Y5 Y6 R5 Y7 R6 F4 F5 D2 R7 P5 P4 "
    "F2 F3 D1 F6 F7 D3 F0 F1 D0",
}
NEAR = {8: 3}
RETURNS = {8: (5, 4, 6, 7, 3, 2, 1, 0)}
NT = (((1,), (1,)), ((), ()))
TN = (((0,), (0,)), ((), ()))


def layer_kernel(
    sp_size,
    cap,
    ids, weights, outer, inner, convin, taps,
    cotangent, stream, w_gate, w_up, w_down, w_out,
    g_gate, g_up, g_down, g_out, g_outer, g_inner, g_convin,
    xall, call, scaled, wgu, wd, wo,
    snd, full_snd, wide_snd, rows, hid, dgu, part,
    gotup, gotdown, relays, sums, share, ret, moe, wall, mall, dsend, dgot,
    ext, dext, mixer, conv, gp, cbuf, hx, xbuf, hz, zsum,
    local, xs, xr, ws, wr, ys, yr, rs, rr, ps, pr, as_, ar, hs, hr, cs, cr, gs, gr, ts, tr,
):
    me = Place(sp_size)
    plane, depth = me.plane, me.depth
    tokens, width = call.shape
    quarter = width // NY
    hidden = wd.shape[0]
    chunk = plane * cap
    half = chunk // 2
    slots = depth * chunk
    distances = [0] + me.dz
    after, before = ((me.sp + 1) % sp_size, me.y), ((me.sp + sp_size - 1) % sp_size, me.y)
    others = [(i, k) for i in range(depth) for k in range(plane) if i + k > 0]
    near = NEAR[depth]
    sent = []
    groups = []

    def columns(y):
        return pl.ds(pl.multiple_of(y * quarter, quarter), quarter)

    def send(src, dst, send_sem, recv_sem, where):
        copy = remote(src, dst, send_sem, recv_sem, where)
        copy.start()
        sent.append(copy)
        return copy

    loads = [
        pltpu.make_async_copy(stream, xall, local.at[0]),
        pltpu.make_async_copy(cotangent, call, local.at[1]),
        pltpu.make_async_copy(w_gate, wgu.at[:, pl.ds(0, hidden)], local.at[2]),
        pltpu.make_async_copy(w_up, wgu.at[:, pl.ds(hidden, hidden)], local.at[3]),
        pltpu.make_async_copy(w_down, wd, local.at[4]),
        pltpu.make_async_copy(w_out, wo, local.at[5]),
    ]
    for copy in loads:
        copy.start()

    barrier = pltpu.get_barrier_semaphore()
    partners = [me.at(distances[i], k) for i, k in others] + [me.in_y(y) for y in (me.up, me.across, me.down)]
    for where in partners:
        pl.semaphore_signal(barrier, inc=1, device_id=where, device_id_type=MESH)

    layers = depth // NY
    holder = me.z // layers == me.y
    for k in range(depth):
        where = (k * plane + me.a, me.z // layers)

        @pl.when(jnp.logical_not(jnp.logical_and(holder, me.z == k)))
        def _():
            pl.semaphore_signal(barrier, inc=1, device_id=where, device_id_type=MESH)

    greetings = len(partners) + depth - holder.astype(jnp.int32)

    def iota(shape, dim):
        return lax.broadcasted_iota(jnp.int32, shape, dim)

    square = (tokens, tokens)
    row, col = iota(square, 0), iota(square, 1)
    ids_row = ids[...]
    upright = [
        jnp.broadcast_to(a[k : k + 1, :], (128, tokens)).T
        for a in (ids_row.astype(F32), weights[...])
        for k in range(2)
    ]
    ids_col = [a[:, :1].astype(jnp.int32) for a in upright[:2]]
    weight_col = [a[:, :1] for a in upright[2:]]
    by_col = [
        (iota((tokens, sp_size), 1) == ids_col[k]).astype(F32) for k in range(2)
    ]
    by_row = [
        (iota((sp_size, tokens), 0) == ids_row[k : k + 1, :]).astype(F32) for k in range(2)
    ]
    count_col = jnp.dot(
        (col < row).astype(F32).astype(BF16), (by_col[0] + by_col[1]).astype(BF16),
        preferred_element_type=F32,
    )
    count_row = jnp.dot(
        (by_row[0] + by_row[1]).astype(BF16), (row < col).astype(F32).astype(BF16),
        preferred_element_type=F32,
    )
    place_col, place_row = [], []
    for k in range(2):
        rank = jnp.sum(by_col[k] * count_col, axis=1, keepdims=True).astype(jnp.int32)
        place_col.append(ids_col[k] * cap + rank)
        rank = jnp.sum(by_row[k] * count_row, axis=0, keepdims=True).astype(jnp.int32)
        place_row.append(ids_row[k : k + 1, :] * cap + rank)

    mixed = inner[...].astype(F32) * convin[...].astype(F32)
    ext[pl.ds(8, tokens), :] = mixed

    loads[0].wait()
    loads[1].wait()
    for k in range(2):
        scaled[pl.ds(k * tokens, tokens), :] = (
            weight_col[k] * call[...].astype(F32)
        ).astype(BF16)

    def base(i):
        return ((me.z + distances[i]) % depth) * chunk

    def build(i):
        slot = base(i) + iota((chunk, tokens), 0)
        hits = [(slot == place_row[k]).astype(F32) for k in range(2)]
        both = (hits[0] + hits[1]).astype(BF16)
        apart = jnp.concatenate(hits, axis=1).astype(BF16)
        here = columns(me.y)
        if i == 0:
            picked = jnp.dot(both, xall[...], preferred_element_type=F32).astype(BF16)
            full_snd[:, 0] = picked.reshape(plane, cap, width)
            picked = jnp.dot(apart, scaled[...], preferred_element_type=F32).astype(BF16)
            full_snd[:, 1] = picked.reshape(plane, cap, width)
            return
        if i < near:
            picked = jnp.dot(both, xall[...], preferred_element_type=F32).astype(BF16)
            wide_snd[i - 1] = picked.reshape(plane, cap, width)
        else:
            picked = jnp.dot(both, xall[:, here], preferred_element_type=F32).astype(BF16)
            snd[i, :, 0] = picked.reshape(plane, cap, quarter)
        picked = jnp.dot(apart, scaled[:, here], preferred_element_type=F32).astype(BF16)
        snd[i, :, 1] = picked.reshape(plane, cap, quarter)

    def group(i, sends, out_of, send_sem, recv_sem):
        for k in range(plane):
            if i + k > 0:
                src, dst = sends(k)
                remote(src, dst, send_sem, recv_sem, me.at(*out_of(k))).start()

    def whole(ref, send_sem, recv_sem):
        return remote(ref, ref, send_sem, recv_sem, me.in_y(me.up))

    def block(i, k):
        return pl.ds((i * plane + k) * cap, cap)

    def blocks(i):
        return pl.ds(cap, chunk - cap) if i == 0 else pl.ds(i * chunk, chunk)

    def those(ref, i):
        return ref.at[0, pl.ds(0, plane - 1)] if i == 0 else ref.at[i]

    def outward(i):
        return lambda k: (distances[i], k)

    def ship(i):
        if i < near:
            def sends(k):
                target = (me.a + k) % plane
                return snd.at[i, target, 1], rows.at[1, block(i, k), columns(me.y)]
        else:
            def sends(k):
                target = (me.a + k) % plane
                return snd.at[i, target], rows.at[:, block(i, k), columns(me.y)]
        group(i, sends, outward(i), xs.at[i], xr.at[i])
        ref = snd.at[:, :, 1] if i < near else snd
        groups.append(whole(those(ref, i), xs.at[i], xr.at[i]))

    def ship_wide(i):
        def sends(k):
            target = (me.a + k) % plane
            if i == 0:
                return full_snd.at[target], rows.at[:, block(i, k), :]
            return wide_snd.at[i - 1, target], rows.at[0, block(i, k), :]

        group(i, sends, outward(i), ws.at[i], wr.at[i])
        sent_refs = full_snd.at[pl.ds(0, plane - 1)] if i == 0 else wide_snd.at[i - 1]
        groups.append(whole(sent_refs, ws.at[i], wr.at[i]))
        if i == 0:
            rows[:, pl.ds(0, cap), :] = full_snd[me.a]

    for i in range(depth):
        build(i)
    loads[5].wait()
    pl.semaphore_wait(barrier, greetings)

    direct, relayed = {}, {}

    def round_y(i):
        arrays = 1 if i < near else slice(None)
        whole(rows.at[arrays, blocks(i), columns(me.y)], xs.at[i], xr.at[i]).wait_recv()
        here = rows.at[arrays, pl.ds(i * chunk, chunk), columns(me.y)]
        for j, y in enumerate((me.up, me.down)):
            direct[i, j] = send(here, here, ys.at[i, j], yr.at[i, j], me.in_y(y))

    def relay(i):
        for j, (origin, target) in enumerate(((me.down, me.up), (me.up, me.down))):
            direct[i, j].wait_recv()
            if i < near:
                piece = rows.at[1, pl.ds(i * chunk + j * half, half), columns(origin)]
            else:
                piece = rows.at[j, pl.ds(i * chunk, chunk), columns(origin)]
            relayed[i, j] = send(piece, piece, ys.at[i, 2 + j], yr.at[i, 2 + j], me.in_y(target))

    def finish(i):
        if i > 0:
            for j in range(2):
                relayed[i, j].wait_recv()
        if i < near:
            arrays = slice(None) if i == 0 else 0
            whole(rows.at[arrays, blocks(i), :], ws.at[i], wr.at[i]).wait_recv()

    ready = []

    def expert(g):
        if not ready:
            ready.append(True)
            for k in range(2, 5):
                loads[k].wait()
        here = pl.ds(g * 2 * chunk, 2 * chunk)
        both = jnp.dot(rows[0, here, :], wgu[...], preferred_element_type=F32)
        gate, up = both[:, :hidden], both[:, hidden:]
        d_hidden = lax.dot_general(rows[1, here, :], wd[...], NT, preferred_element_type=F32)
        sig = jax.nn.sigmoid(gate)
        silu = gate * sig
        hid[here, :] = (silu * up).astype(BF16)
        dgu[here, pl.ds(0, hidden)] = (d_hidden * up * sig * (1.0 + gate * (1.0 - sig))).astype(BF16)
        dgu[here, pl.ds(hidden, hidden)] = (d_hidden * silu).astype(BF16)
        part[here, :] = lax.dot_general(
            dgu[here, :], wgu[...], NT, preferred_element_type=F32
        ).astype(BF16)

    got = {}

    def first(i):
        low, high = pl.ds(i * chunk, half), pl.ds(i * chunk + half, half)
        lo, hi = pl.ds(0, half), pl.ds(half, half)
        for j, src, dst, y in (
            (0, part.at[low, columns(me.across)], relays.at[i, 0], me.down),
            (1, part.at[high, columns(me.across)], relays.at[i, 1], me.up),
            (2, part.at[high, columns(me.down)], gotup.at[i, hi], me.down),
            (3, part.at[low, columns(me.up)], gotdown.at[i, lo], me.up),
        ):
            got[i, j] = send(src, dst, rs.at[i, j], rr.at[i, j], me.in_y(y))

    channels = mixer.shape[1]

    def lanes(y):
        return pl.ds(pl.multiple_of(y * channels, channels), channels)

    def to_others(kind, src_of, dst):
        for o in range(1, NY):
            y = (me.y + o) % NY
            exchanged[kind, o] = send(
                src_of(y), dst(o), as_.at[kind, o - 1], ar.at[kind, o - 1], me.in_y(y)
            )

    exchanged = {}

    def share_weights(_):
        exchanged["halo"] = send(
            ext.at[pl.ds(tokens, 8)], ext.at[pl.ds(0, 8)], hs.at[0], hr.at[0], after
        )
        to_others(0, lambda y: wo.at[columns(y), :], lambda o: wall.at[:, lanes(me.y)])
        wall[:, lanes(me.y)] = wo[columns(me.y), :]

    def convolution(_):
        exchanged["halo"].wait_recv()
        ext[pl.ds(0, 8), :] = jnp.where(me.sp == 0, 0.0, ext[pl.ds(0, 8), :])
        conv_out = (
            taps[0:1, :] * ext[pl.ds(6, tokens), :]
            + taps[1:2, :] * ext[pl.ds(7, tokens), :]
            + taps[2:3, :] * ext[pl.ds(8, tokens), :]
        )
        conv[...] = conv_out
        mixer_out = (outer[...].astype(F32) * conv_out).astype(BF16)
        mixer[...] = mixer_out
        mall[:, lanes(me.y)] = mixer_out
        to_others(1, lambda y: mixer, lambda o: mall.at[:, lanes(me.y)])

    jobs = {
        "S": ship, "X": ship_wide, "Y": round_y, "R": relay, "F": finish, "D": expert, "P": first,
        "W": share_weights, "C": convolution,
    }
    for name in ORDERS[depth].split():
        jobs[name[0]](int(name[1:]))

    def second(i):
        low, high = pl.ds(i * chunk, half), pl.ds(i * chunk + half, half)
        lo, hi = pl.ds(0, half), pl.ds(half, half)
        for j, mine, y, dst in (
            (0, low, me.down, gotup.at[i, lo]),
            (1, high, me.up, gotdown.at[i, hi]),
        ):
            got[i, j].wait_recv()
            sums[i, j] = (
                part[mine, columns(y)].astype(F32) + relays[i, j].astype(F32)
            ).astype(BF16)
            got[i, 4 + j] = send(sums.at[i, j], dst, rs.at[i, 4 + j], rr.at[i, 4 + j], me.in_y(y))

    def third(i):
        for j in range(2, 6):
            got[i, j].wait_recv()
        total = (
            part[pl.ds(i * chunk, chunk), columns(me.y)].astype(F32)
            + gotup[i].astype(F32)
            + gotdown[i].astype(F32)
        ).astype(BF16)
        share[i] = total.reshape(plane, cap, quarter)
        if i == 0:
            ret[0, me.a] = share[0, 0]

        def sends(k):
            return share.at[i, k], ret.at[i, me.a]

        group(i, sends, lambda k: (depth - distances[i], plane - k), ps.at[i], pr.at[i])
        groups.append(whole(those(share, i), ps.at[i], pr.at[i]))

    def fourth(i):
        whole(those(ret, i), ps.at[i], pr.at[i]).wait_recv()
        slot = base(i) + iota((tokens, chunk), 1)
        hit = ((slot == place_col[0]) | (slot == place_col[1])).astype(F32).astype(BF16)
        moe[...] += jnp.dot(hit, ret[i].reshape(chunk, quarter), preferred_element_type=F32)

    tiles = depth
    wide = width // tiles

    def weight_grads(t):
        cols = pl.ds(t * wide, wide)
        both = lax.dot_general(rows[0, :, cols], dgu[...], TN, preferred_element_type=F32)
        g_gate[0, cols, :] = both[:, :hidden].astype(BF16)
        g_up[0, cols, :] = both[:, hidden:].astype(BF16)
        g_down[0, :, cols] = lax.dot_general(
            hid[...], rows[1, :, cols], TN, preferred_element_type=F32
        ).astype(BF16)

    order = RETURNS[depth]
    moe[...] = call[:, columns(me.y)].astype(F32)
    early = 2
    for step in range(depth + 1):
        if step + 2 < depth and step + 2 >= early:
            first(order[step + 2])
        if step < depth:
            second(order[step])
        if step >= 1:
            third(order[step - 1])
        if step < tiles:
            weight_grads(step)
    for k in range(depth):
        fourth(order[k])

    for o in range(1, NY):
        exchanged[1, o].wait_recv()
        exchanged[0, o].wait_recv()
    stream_grad = moe[...].astype(BF16)
    core = me.a % 2
    across_x = me.a // 2
    chips = plane // 2
    gp[...] = (
        lax.dot_general(stream_grad, mall[...], TN, preferred_element_type=F32)
        .astype(BF16)
        .reshape(gp.shape)
    )
    between = send(
        gp.at[:, :, 1 - core], cbuf, cs.at[0], cr.at[0],
        (me.z * plane + across_x * 2 + 1 - core, me.y),
    )
    for o in range(1, NY):
        y = (me.y + o) % NY
        dsend[o - 1] = jnp.dot(
            stream_grad, wall[:, lanes(y)], preferred_element_type=F32
        ).astype(BF16)
    to_others(2, lambda y: dsend.at[(y - me.y + NY) % NY - 1], lambda o: dgot.at[o - 1])
    d_mixer = jnp.dot(stream_grad, wall[:, lanes(me.y)], preferred_element_type=F32)

    between.wait_recv()
    summed = gp[:, :, core].astype(F32) + cbuf[...].astype(F32)
    hx[...] = summed.astype(BF16)
    over_x = []
    for d in range(1, chips):
        target = (across_x + d) % chips
        over_x.append(
            send(
                hx.at[:, target], xbuf.at[d - 1], gs.at[d - 1], gr.at[d - 1],
                (me.z * plane + target * 2 + core, me.y),
            )
        )

    for o in range(1, NY):
        exchanged[2, o].wait_recv()
        d_mixer += dgot[o - 1].astype(F32)
    dext[pl.ds(0, tokens), :] = d_mixer * outer[...].astype(F32)
    trail = send(dext.at[pl.ds(0, 8)], dext.at[pl.ds(tokens, 8)], hs.at[1], hr.at[1], before)
    g_outer[...] = d_mixer * conv[...]

    summed = hx[:, across_x].astype(F32)
    for d in range(1, chips):
        over_x[d - 1].wait_recv()
        summed += xbuf[d - 1].astype(F32)
    to_owner = []
    for k in range(layers):
        for y in range(NY):
            hz[k, y] = summed[k, :, y * channels : (y + 1) * channels].astype(BF16)
            owner = layers * me.y + k
            mine = jnp.logical_and(owner == me.z, me.y == y)
            copy = remote(
                hz.at[k, y], zsum.at[me.z], ts.at[k, y], tr.at[me.z], (owner * plane + me.a, y)
            )
            to_owner.append((mine, copy))

            @pl.when(mine)
            def _():
                zsum[me.z] = hz[k, y]

            @pl.when(jnp.logical_not(mine))
            def _():
                copy.start()

    trail.wait_recv()
    dext[pl.ds(tokens, 8), :] = jnp.where(me.sp == sp_size - 1, 0.0, dext[pl.ds(tokens, 8), :])
    d_mixed = (
        taps[2:3, :] * dext[pl.ds(0, tokens), :]
        + taps[1:2, :] * dext[pl.ds(1, tokens), :]
        + taps[0:1, :] * dext[pl.ds(2, tokens), :]
    )
    g_inner[...] = d_mixed * convin[...].astype(F32)
    g_convin[...] = d_mixed * inner[...].astype(F32)

    for k in range(depth):
        @pl.when(jnp.logical_not(jnp.logical_and(holder, me.z == k)))
        def _():
            remote(zsum.at[k], zsum.at[k], ts.at[0, 0], tr.at[k], me.in_y(me.up)).wait_recv()

    total = zsum[0].astype(F32)
    for k in range(1, depth):
        total += zsum[k].astype(F32)
    g_out[...] = total
    for copy in sent + groups:
        copy.wait_send()
    for mine, copy in to_owner:
        @pl.when(jnp.logical_not(mine))
        def _():
            copy.wait_send()


def shards(
    out_cotangent,
    stream,
    route_ids,
    route_weights,
    gate_proj,
    up_proj,
    down_proj,
    outer_gate,
    inner_gate,
    conv_input,
    conv_taps,
    out_proj,
):
    sp = lax.axis_size("sp")
    plane = plane_size(sp)
    depth = sp // plane
    tokens, width = stream.shape
    cap = 4 * tokens // sp
    chunk = plane * cap
    slots = depth * chunk
    quarter = width // NY
    hidden = gate_proj.shape[2]
    channels = outer_gate.shape[1]
    layers = depth // NY
    chips = plane // 2
    near = NEAR[depth]
    block = width // sp
    vmem = pl.BlockSpec(memory_space=pltpu.VMEM)
    hbm = pl.BlockSpec(memory_space=pl.ANY)

    def dma(*shape):
        return pltpu.SemaphoreType.DMA(shape)

    def bf16(*shape):
        return pltpu.VMEM(shape, BF16)

    def f32(*shape):
        return pltpu.VMEM(shape, F32)

    shapes = (
        ((1, width, hidden), BF16),
        ((1, width, hidden), BF16),
        ((1, hidden, width), BF16),
        ((block, channels), F32),
        ((tokens, channels), F32),
        ((tokens, channels), F32),
        ((tokens, channels), F32),
    )
    return pl.pallas_call(
        functools.partial(layer_kernel, sp, cap),
        name="layer",
        out_shape=tuple(pltpu.VMEM(*s) for s in shapes),
        in_specs=[vmem] * 6 + [hbm] * 6,
        out_specs=(vmem,) * 7,
        scratch_shapes=[
            bf16(tokens, width),
            bf16(tokens, width),
            bf16(2 * tokens, width),
            bf16(width, 2 * hidden),
            bf16(hidden, width),
            bf16(width, channels),
            bf16(depth, plane, 2, cap, quarter),
            bf16(plane, 2, cap, width),
            bf16(max(near - 1, 1), plane, cap, width),
            bf16(2, slots, width),
            bf16(slots, hidden),
            bf16(slots, 2 * hidden),
            bf16(slots, width),
            bf16(depth, chunk, quarter),
            bf16(depth, chunk, quarter),
            bf16(depth, 2, chunk // 2, quarter),
            bf16(depth, 2, chunk // 2, quarter),
            bf16(depth, plane, cap, quarter),
            bf16(depth, plane, cap, quarter),
            f32(tokens, quarter),
            bf16(quarter, NY * channels),
            bf16(tokens, NY * channels),
            bf16(NY - 1, tokens, channels),
            bf16(NY - 1, tokens, channels),
            f32(tokens + 8, channels),
            f32(tokens + 8, channels),
            bf16(tokens, channels),
            f32(tokens, channels),
            bf16(layers, chips, 2, block, NY * channels),
            bf16(layers, chips, block, NY * channels),
            bf16(layers, chips, block, NY * channels),
            bf16(max(chips - 1, 1), layers, block, NY * channels),
            bf16(layers, NY, block, channels),
            bf16(depth, block, channels),
            dma(6),
            dma(depth),
            dma(depth),
            dma(near),
            dma(near),
            dma(depth, 4),
            dma(depth, 4),
            dma(depth, 6),
            dma(depth, 6),
            dma(depth),
            dma(depth),
            dma(3, NY - 1),
            dma(3, NY - 1),
            dma(2),
            dma(2),
            dma(1),
            dma(1),
            dma(max(chips - 1, 1)),
            dma(max(chips - 1, 1)),
            dma(layers, NY),
            dma(depth),
        ],
        compiler_params=pltpu.CompilerParams(
            collective_id=0, has_side_effects=True, vmem_limit_bytes=60 * 1024 * 1024
        ),
    )(
        route_ids.T, route_weights.T, outer_gate, inner_gate, conv_input, conv_taps,
        out_cotangent, stream, gate_proj[0], up_proj[0], down_proj[0], out_proj,
    )


def solution(mesh):
    placed = (
        P("sp", None),
        P("sp", None),
        P("sp", None),
        P("sp", None),
        P("sp", None, "tp"),
        P("sp", None, "tp"),
        P("sp", "tp", None),
        P("sp", "tp"),
        P("sp", "tp"),
        P("sp", "tp"),
        P(None, "tp"),
        P(None, "tp"),
    )
    return jax.shard_map(
        shards,
        mesh=mesh,
        in_specs=placed,
        out_specs=(
            P("sp", None, "tp"),
            P("sp", None, "tp"),
            P("sp", "tp", None),
            P("sp", "tp"),
            P("sp", "tp"),
            P("sp", "tp"),
            P("sp", "tp"),
        ),
        check_vma=False,
    )
```
